256 devices in a mesh: kv: 32 (over z, x), tp: 8 (over y, core).
Axes of the slice: x: 4, y: 4, z: 8, core: 2. Of those that a mesh axis runs over, the one named last changes fastest.
Arguments:
- tokens: bfloat16 [384, 2048], P(None, 'kv'), may hold values from -40 to 40
- norm_gain: float32 [2048], P('kv'), may hold values from 0.1 to 1.9
- w_query: bfloat16 [2048, 1024], P('kv', 'tp'), may hold values from -0.088388348 to 0.088388348
- w_key: bfloat16 [2048, 1024], P('kv', 'tp'), may hold values from -0.125 to 0.125
- w_value: bfloat16 [2048, 1024], P('kv', 'tp'), may hold values from -0.125 to 0.125
- w_gate: bfloat16 [2048, 16], replicated, may hold values from -0.125 to 0.125
- gate_bias: float32 [16], replicated, may hold values from -1 to 3
- w_out: bfloat16 [1024, 2048], P('tp', 'kv'), may hold values from -0.1875 to 0.1875
- keys_cache: bfloat16 [24, 16384, 1024], P(None, 'kv', 'tp'), may hold values from -512 to 512
- values_cache: bfloat16 [24, 16384, 1024], P(None, 'kv', 'tp'), may hold values from -6 to 6
- cum_gates: float32 [24, 16, 16384], P(None, 'tp', 'kv'), may hold values from -16784 to 0, as said below
- prior_len: int32 [24], replicated, may hold values from 8192 to 16362, as said below
- accepted: int32 [24], replicated, may hold values from 0 to 6
- parents: int32 [24, 16], replicated, may hold values from -1 to 14, as said below
Outputs:
- mixed_rows: bfloat16 [384, 2048], P('tp', 'kv')
- keys_out: bfloat16 [24, 16384, 1024], P(None, 'kv', 'tp')
- values_out: bfloat16 [24, 16384, 1024], P(None, 'kv', 'tp')
The draws below stay inside these ranges and needn't reach their ends.
Inputs may be any that keep to these rules, and one draw needn't show every extreme that they name: parents[b, 0] = -1 and 0 <= parents[b, j] < j for later j. prior_len is at least half of 16384, and prior_len + accepted + 16 <= 16384. `cum_gates`: non-increasing along positions.
All inputs are finite; a program needn't handle non-finite values.
Results may differ from the reference program's by a relative error of at most 0.04.
Values may be sent and summed in bfloat16 or wider, within the bound.
A program may use at most 64 MiB of HBM per device.

```python
import jax
import jax.numpy as jnp
from jax import lax

D = 2048
H = 16
HEAD = 64
PROPS = 16
MOST_ACCEPTED = 6
SEQUENCE_TOTAL = 24
LEN_DEV = 512
CACHE_POSITIONS = 16384
ROWS = 384
N_KV = 32
N_TP = 8


def token_floats(token_key):
    random_keys = jax.random.split(token_key, 3)
    normal_part = jax.random.normal(random_keys[0], (ROWS, D), jnp.float32)
    row_scale = jnp.exp(jax.random.uniform(random_keys[1], (ROWS, 1), jnp.float32, jnp.log(0.3), jnp.log(3.0)))
    column_rise = jnp.exp(jnp.log(3.0) * jnp.arange(D, dtype=jnp.float32)[None, :] / D)
    column_spread = jnp.exp(jax.random.uniform(random_keys[2], (1, D), jnp.float32, jnp.log(0.5), jnp.log(2.0)))
    return jnp.clip(normal_part * row_scale * column_rise * column_spread, -40.0, 40.0)


def query_floats(weight_key):
    drawn = jax.random.truncated_normal(weight_key, -4.0, 4.0, (D, H * HEAD), jnp.float32)
    return drawn * D ** (-0.5)


def draw_tokens(key, part):
    return token_floats(jax.random.fold_in(key, 101)).astype(jnp.bfloat16)


def draw_w_query(key, part):
    return query_floats(jax.random.fold_in(key, 202)).astype(jnp.bfloat16)


def draw_keys_cache(key, part):
    random_keys = jax.random.split(jax.random.fold_in(key, 303), 1)
    result = jax.random.normal(random_keys[0], (SEQUENCE_TOTAL, CACHE_POSITIONS, H * HEAD), jnp.float32)
    result = jnp.clip(result, -6.0, 6.0)
    return jnp.clip(result, -512.0, 512.0).astype(jnp.bfloat16)


def draw_cum_gates(key, part):
    random_keys = jax.random.split(key, 8)
    ranking = jax.random.permutation(random_keys[0], H)
    quick_count = H // 2
    fast_decay_heads = (ranking < quick_count)[None, :, None]
    quick_rate = jnp.exp(jax.random.uniform(random_keys[1], (SEQUENCE_TOTAL, H, 1), jnp.float32, jnp.log(1.0 / 100.0), jnp.log(1.0 / 30.0)))
    slow_rate = jnp.exp(jax.random.uniform(random_keys[2], (SEQUENCE_TOTAL, H, 1), jnp.float32, jnp.log(0.1), jnp.log(0.4))) / CACHE_POSITIONS
    decay_rates = jnp.where(fast_decay_heads, quick_rate, slow_rate)
    block_count = CACHE_POSITIONS // LEN_DEV
    block_multiplier = jnp.exp(jax.random.uniform(random_keys[3], (SEQUENCE_TOTAL, 1, block_count, 1), jnp.float32, 0.0, jnp.log(4.0)))
    block_multiplier = jnp.broadcast_to(block_multiplier, (SEQUENCE_TOTAL, 1, block_count, LEN_DEV)).reshape(SEQUENCE_TOTAL, 1, CACHE_POSITIONS)
    jitter_level = jax.random.uniform(random_keys[4], (SEQUENCE_TOTAL, H, CACHE_POSITIONS), jnp.float32, 0.4, 1.6)
    spike_position = jax.random.randint(random_keys[5], (SEQUENCE_TOTAL, 1, CACHE_POSITIONS), 0, CACHE_POSITIONS) < 2
    dropped_fraction = jax.random.uniform(random_keys[6], (SEQUENCE_TOTAL, H, CACHE_POSITIONS), jnp.float32, 0.2, 0.5)
    spike_events = jnp.where(spike_position & jnp.logical_not(fast_decay_heads), jnp.log(1.0 - dropped_fraction), 0.0)
    gate_increments = spike_events - decay_rates * block_multiplier * jitter_level
    head_offset = jax.random.uniform(random_keys[7], (SEQUENCE_TOTAL, H, 1), jnp.float32, 0.0, 320.0)
    return (jnp.cumsum(gate_increments, axis=2) - head_offset).astype(jnp.float32)


def draw_prior_len(key, part):
    return jax.random.randint(key, (SEQUENCE_TOTAL,), CACHE_POSITIONS // 2, CACHE_POSITIONS - PROPS - MOST_ACCEPTED + 1, dtype=jnp.int32)


def draw_parents(key, part):
    columns = jnp.arange(PROPS, dtype=jnp.int32)
    random_bits = jax.random.randint(key, (SEQUENCE_TOTAL, PROPS), 0, 1 << 20, dtype=jnp.int32)
    picked = random_bits % jnp.maximum(columns, 1)[None, :]
    return jnp.where(columns[None, :] == 0, -1, picked).astype(jnp.int32)


def set_ends(values, own_key, smallest, largest):
    place = [jax.random.randint(jax.random.fold_in(own_key, axis), (), 0, length) for axis, length in enumerate(values.shape)]
    longest = values.shape.index(max(values.shape))
    next_to = place[:longest] + [(place[longest] + 1) % values.shape[longest]] + place[longest + 1:]
    return values.at[tuple(place)].set(smallest).at[tuple(next_to)].set(largest)


def steps_of(key, shape, pieces, least, high):
    loudness = 1.0
    for axis_at, parts in pieces:
        heights = jax.random.uniform(jax.random.fold_in(jax.random.fold_in(key, 6), axis_at), (parts,), jnp.float32, least / len(pieces), high / len(pieces))
        loudness = loudness * jnp.repeat(jnp.exp(heights), shape[axis_at] // parts).reshape((-1,) + (1,) * (len(shape) - 1 - axis_at))
    return loudness


def centred(stream_key, extent, spread, limit, cuts=(), held_as=jnp.bfloat16):
    values = jax.random.normal(stream_key, extent, jnp.float32) * spread
    if len(cuts) > 0:
        values = steps_of(stream_key, extent, cuts, -0.22, 0.18) * values
    return jnp.clip(values, min=-limit, max=limit).astype(held_as)


def setup_inputs(seed: int = 0) -> dict:
    streams_of = jax.random.split(jax.random.key(seed), 15)
    tokens = draw_tokens(jax.random.fold_in(streams_of[14], 71), 0)
    norm_gain = jnp.clip(1.0 + 0.18 * jax.random.normal(streams_of[1], (D,), jnp.float32), 0.1, 1.9)
    w_query = draw_w_query(jax.random.fold_in(streams_of[14], 71), 0)
    w_key = centred(streams_of[3], (D, H * HEAD), D ** -0.5, 0.125, ((0, 32), (1, 8)))
    w_value = centred(streams_of[4], (D, H * HEAD), D ** -0.5, 0.125, ((0, 32), (1, 8)))
    w_gate = centred(streams_of[5], (D, H), D ** -0.5, 0.125)
    gate_bias = jnp.clip(jax.random.uniform(streams_of[6], (H,), jnp.float32, -1.0, 3.0), -1.0, 3.0)
    w_out = centred(streams_of[7], (H * HEAD, D), (H * HEAD) ** -0.5, 0.1875, ((0, 8), (1, 32)))
    keys_cache = draw_keys_cache(jax.random.fold_in(streams_of[14], 71), 0)
    values_cache = centred(streams_of[9], (SEQUENCE_TOTAL, CACHE_POSITIONS, H * HEAD), 1.0, 6.0, ((1, 32), (2, 8)))
    cum_gates = draw_cum_gates(jax.random.fold_in(streams_of[14], 71), 0)
    prior_len = draw_prior_len(jax.random.fold_in(streams_of[14], 71), 0)
    accepted = set_ends(jax.random.randint(streams_of[12], (SEQUENCE_TOTAL,), 0, MOST_ACCEPTED + 1), jax.random.fold_in(streams_of[12], 1), 0, MOST_ACCEPTED).astype(jnp.int32)
    parents = draw_parents(jax.random.fold_in(streams_of[14], 71), 0)
    return {"tokens": tokens, "norm_gain": norm_gain, "w_query": w_query, "w_key": w_key, "w_value": w_value, "w_gate": w_gate, "gate_bias": gate_bias, "w_out": w_out, "keys_cache": keys_cache, "values_cache": values_cache, "cum_gates": cum_gates, "prior_len": prior_len, "accepted": accepted, "parents": parents}


masked_score = -1e+30
norm_eps = 1e-06

def ancestry(parents):
    columns = jnp.arange(PROPS, dtype=jnp.int32)
    parent_link = (parents[:, :, None] == columns[None, None, :]).astype(jnp.float32)
    reached = jnp.eye(PROPS, dtype=jnp.float32)[None] + parent_link
    for squaring in range(PROPS.bit_length()):
        reached = jnp.minimum(jnp.einsum('bij,bjk->bik', reached, reached, precision=lax.Precision.HIGHEST), 1.0)
    return reached

def reference(tokens, norm_gain, w_query, w_key, w_value, w_gate, gate_bias, w_out, keys_cache, values_cache, cum_gates, prior_len, accepted, parents):
    floats = tokens.astype(jnp.float32)
    inv_rms = lax.rsqrt(lax.optimization_barrier(jnp.sum(floats * floats, axis=1)) / D + norm_eps)
    scaled = (floats * norm_gain).astype(jnp.bfloat16)

    def project(weight):
        return inv_rms[:, None] * jnp.dot(scaled, weight, preferred_element_type=jnp.float32)
    queries = project(w_query).astype(jnp.bfloat16)
    new_keys = project(w_key).astype(jnp.bfloat16)
    new_values = project(w_value).astype(jnp.bfloat16)
    log_gates = jax.nn.log_sigmoid(project(w_gate) + gate_bias).reshape(SEQUENCE_TOTAL, PROPS, H)
    reached = ancestry(parents)
    tree_gates = jnp.einsum('bij,bjh->bih', reached, log_gates, precision=lax.Precision.HIGHEST)
    filled = prior_len + accepted
    last_pos = filled - 1
    index_last = jnp.broadcast_to(last_pos[:, None, None], (SEQUENCE_TOTAL, H, 1))
    last_gate = jnp.take_along_axis(cum_gates, index_last, axis=2)[:, :, 0]
    prop_cum = last_gate[:, None, :] + tree_gates
    owners = (last_pos // LEN_DEV).astype(jnp.int32)
    scale = HEAD ** (-0.5)

    def attend(packed):
        seq_query, seq_keys, seq_values, seq_cum, seq_newk, seq_newv, seq_prop, seq_reach, seq_fill, seq_owner = packed
        query_f = seq_query.reshape(PROPS, H, HEAD).astype(jnp.float32)
        keys_f = seq_keys.reshape(CACHE_POSITIONS, H, HEAD).astype(jnp.float32)
        scores = jnp.einsum('ihd,phd->hip', query_f, keys_f) * scale - seq_cum[:, None, :]
        positions = jnp.arange(CACHE_POSITIONS, dtype=jnp.int32)
        valid_keys = positions < seq_fill
        scores = jnp.where(valid_keys[None, None, :], scores, masked_score)
        blocked = scores.reshape(H, PROPS, N_KV, LEN_DEV)
        newk_f = seq_newk.reshape(PROPS, H, HEAD).astype(jnp.float32)
        tree_scores = jnp.einsum('ihd,jhd->hij', query_f, newk_f) * scale - jnp.transpose(seq_prop)[:, None, :]
        tree_live = (seq_reach > 0.5)[None]
        tree_scores = jnp.where(tree_live, tree_scores, masked_score)
        is_owner = jnp.arange(N_KV, dtype=jnp.int32) == seq_owner
        block_max = lax.optimization_barrier(jnp.max(blocked, axis=3))
        tree_max = lax.optimization_barrier(jnp.max(tree_scores, axis=2))
        block_max = jnp.where(is_owner[None, None, :], jnp.maximum(block_max, tree_max[:, :, None]), block_max)
        owner_max = lax.optimization_barrier(jnp.max(jnp.where(is_owner[None, None, :], block_max, masked_score), axis=2))
        valid_blocks = valid_keys.reshape(N_KV, LEN_DEV)[None, None]
        weights = jnp.where(valid_blocks, jnp.exp(blocked - block_max[..., None]), 0.0)
        tree_weights = jnp.where(tree_live, jnp.exp(tree_scores - owner_max[:, :, None]), 0.0)
        block_sums = lax.optimization_barrier(jnp.sum(weights, axis=3)) + jnp.where(is_owner[None, None, :], lax.optimization_barrier(jnp.sum(tree_weights, axis=2))[:, :, None], 0.0)
        values_f = seq_values.reshape(N_KV, LEN_DEV, H, HEAD).astype(jnp.float32)
        newv_f = seq_newv.reshape(PROPS, H, HEAD).astype(jnp.float32)
        rounded = lax.optimization_barrier(weights.astype(jnp.bfloat16)).astype(jnp.float32)
        tree_rounded = lax.optimization_barrier(tree_weights.astype(jnp.bfloat16)).astype(jnp.float32)
        block_values = jnp.einsum('hinp,nphd->hind', rounded, values_f)
        tree_values = jnp.einsum('hij,jhd->hid', tree_rounded, newv_f)
        block_values = block_values + jnp.where(is_owner[None, None, :, None], tree_values[:, :, None, :], 0.0)
        block_values = lax.optimization_barrier(block_values.astype(jnp.bfloat16)).astype(jnp.float32)
        top_score = lax.optimization_barrier(jnp.max(block_max, axis=2))
        rescale = jnp.exp(block_max - top_score[..., None])
        grand_total = lax.optimization_barrier(jnp.sum(rescale * block_sums, axis=2))
        result = lax.optimization_barrier(jnp.sum(rescale[..., None] * block_values, axis=2)) / grand_total[..., None]
        return jnp.transpose(result, (1, 0, 2)).astype(jnp.bfloat16)
    packed = (queries.reshape(SEQUENCE_TOTAL, PROPS, H * HEAD), keys_cache, values_cache, cum_gates, new_keys.reshape(SEQUENCE_TOTAL, PROPS, H * HEAD), new_values.reshape(SEQUENCE_TOTAL, PROPS, H * HEAD), prop_cum, reached, filled, owners)
    attended = lax.map(attend, packed).reshape(ROWS, H * HEAD)
    group = H // N_TP * HEAD
    parted = attended.reshape(ROWS, N_TP, group).astype(jnp.float32)
    weight_groups = w_out.reshape(N_TP, group, D).astype(jnp.float32)
    head_parts = jnp.einsum('rgc,gcd->grd', parted, weight_groups)
    head_parts = lax.optimization_barrier(head_parts.astype(jnp.bfloat16)).astype(jnp.float32)
    mixed_rows = lax.optimization_barrier(jnp.sum(head_parts, axis=0)).astype(jnp.bfloat16)

    def write(cache, new_rows, start):
        return lax.dynamic_update_slice(cache, new_rows, (start.astype(jnp.int32), jnp.zeros((), jnp.int32)))
    keys_out = jax.vmap(write)(keys_cache, new_keys.reshape(SEQUENCE_TOTAL, PROPS, H * HEAD), filled)
    values_out = jax.vmap(write)(values_cache, new_values.reshape(SEQUENCE_TOTAL, PROPS, H * HEAD), filled)
    return (mixed_rows, keys_out, values_out)
```

```python
import functools

import jax
import jax.numpy as jnp
from jax import lax
from jax.experimental import pallas as pl
from jax.experimental.pallas import tpu as pltpu
from jax.sharding import PartitionSpec as P

D = 2048
HEAD = 64
PROPS = 16
SEQS = 24
NZ, NX = 8, 4
NKV = NZ * NX
WIDE = 128
MASKED = 1e30
NORM_EPS = 1e-06
FIRST_WRITER = 4

f32, bf16 = jnp.float32, jnp.bfloat16


def iota(shape, dim):
    return lax.broadcasted_iota(jnp.int32, shape, dim)


def dot_nt(a, b):
    return lax.dot_general(a, b, (((1,), (1,)), ((), ())), preferred_element_type=f32)


def dot_nn(a, b):
    return lax.dot_general(a, b, (((1,), (0,)), ((), ())), preferred_element_type=f32)


def far_first(i):
    return 4 + (1 - 2 * lax.rem(i, 2)) * lax.div(i + 1, 2)


def near_first(i):
    odd = lax.rem(i, 2)
    return odd * lax.div(i + 1, 2) + (1 - odd) * lax.rem(NZ - lax.div(i, 2), NZ)


def owner_of(z, r):
    return z * NX + lax.rem(z + 1 + r, NX)


def split_heads(rows):
    lane = iota((2 * PROPS, WIDE), 1)
    sub = iota((2 * PROPS, WIDE), 0)
    both = jnp.concatenate([rows, rows], axis=0)
    return jnp.where((lane < HEAD) == (sub < PROPS), both, 0.0).astype(bf16)


def join_heads(rows):
    lane = iota((PROPS, WIDE), 1)
    return jnp.where(lane < HEAD, rows[:PROPS], rows[PROPS:])


def as_row(tops, sums):
    lane = iota((2 * PROPS, WIDE), 1)
    sub = iota((2 * PROPS, WIDE), 0)
    spread = jnp.where(lane == sub, tops, jnp.where(lane == sub + 2 * PROPS, sums, 0.0))
    return jnp.sum(spread, axis=0, keepdims=True)


def as_column(row, start):
    lane = iota((PROPS, WIDE), 1)
    sub = iota((PROPS, WIDE), 0)
    return jnp.sum(jnp.where(lane == sub + start, row, 0.0), axis=1, keepdims=True)


def step_kernel(
    tp_count,
    tok_hbm,
    gain_hbm,
    wq_hbm,
    wk_hbm,
    wv_hbm,
    wg_hbm,
    wo_hbm,
    keys_hbm,
    values_hbm,
    cum_hbm,
    bias_ref,
    prior_ref,
    accepted_ref,
    parents_ref,
    mixed_ref,
    new_ref,
    tok,
    gain,
    wq,
    wk,
    wv,
    wg,
    wo,
    keys,
    values,
    cum,
    part_q,
    part_n,
    part_s,
    got_q,
    got_n,
    got_s,
    queries,
    own_new,
    out_v,
    out_s,
    got_v,
    got_m,
    attended,
    reach,
    heads_out,
    heads_in,
    local_sems,
    send_sems,
    recv_sems,
    query_sems,
    new_sems,
    att_sems,
):
    me = lax.axis_index("kv")
    tp = lax.axis_index("tp")
    my_z, my_x = lax.div(me, NX), lax.rem(me, NX)
    my_r = lax.rem(my_x - my_z - 1 + 2 * NX * NZ, NX)
    owner = my_r < 3
    own_b = lax.min(3 * my_z + my_r, SEQS - 1)
    length = keys.shape[1]
    offset = me * length
    heads = 2

    barrier = pltpu.get_barrier_semaphore()

    @pl.loop(0, NKV - 1)
    def _(i):
        pl.semaphore_signal(barrier, inc=1, device_id={"kv": lax.rem(me + i + 1, NKV)})

    @pl.loop(0, tp_count - 1)
    def _(i):
        pl.semaphore_signal(barrier, inc=1, device_id={"tp": lax.rem(tp + i + 1, tp_count)})

    gate_block = pl.multiple_of(lax.div(me, 2) * WIDE, WIDE)
    pairs = (
        (tok_hbm, tok),
        (gain_hbm, gain),
        (wg_hbm.at[:, pl.ds(gate_block, WIDE)], wg),
        (wq_hbm, wq),
        (wk_hbm, wk),
        (wv_hbm, wv),
        (cum_hbm, cum),
        (keys_hbm, keys),
        (values_hbm, values),
        (wo_hbm, wo),
    )
    loads = [pltpu.make_async_copy(a, b, local_sems.at[i]) for i, (a, b) in enumerate(pairs)]
    for load in loads:
        load.start()

    @pl.when(owner)
    def _():
        lane = iota((PROPS, WIDE), 1)
        sub = iota((PROPS, WIDE), 0)
        parent = jnp.full((PROPS, WIDE), -1, jnp.int32)
        for j in range(PROPS):
            parent = jnp.where(sub == j, parents_ref[j, own_b], parent)
        seen = jnp.where((lane == sub) | (lane == parent), 1.0, 0.0)
        rest = jnp.zeros((WIDE - PROPS, WIDE), f32)
        for _ in range(4):
            square = jnp.concatenate([seen, rest], axis=0).astype(bf16)
            seen = jnp.minimum(dot_nn(seen.astype(bf16), square), 1.0)
        reach[...] = jnp.concatenate([seen, rest], axis=0)

    for load in loads[:6]:
        load.wait()
    x = tok[...].astype(f32)
    width = x.shape[0]
    eye = iota((width, width), 0) == iota((width, width), 1)
    gain_col = jnp.sum(jnp.where(eye, gain[...], 0.0), axis=1, keepdims=True)
    square_row = jnp.sum(x * x, axis=0, keepdims=True)
    scaled_t = x * gain_col
    scaled = jnp.transpose(scaled_t).astype(bf16)
    gate_w = wg[...].astype(f32)
    gate_w = jnp.where(lax.rem(me, 2) == 0, gate_w[:, :width], gate_w[:, width:]).astype(bf16)
    gates = dot_nn(gate_w, scaled_t.astype(bf16))
    gate_row = iota(gates.shape, 0)
    rows = [square_row] + [
        jnp.sum(jnp.where(gate_row == heads * tp + h, gates, 0.0), axis=0, keepdims=True)
        for h in range(heads)
    ]
    for j in range(3):
        for k, row in enumerate(rows):
            part_s[j, pl.ds(k, 1), :] = row[:, j * WIDE : (j + 1) * WIDE]
        part_s[j, pl.ds(3, 1), :] = jnp.zeros((1, WIDE), f32)
    part_q[...] = dot_nn(scaled, wq[...]).astype(bf16).reshape(SEQS, PROPS, WIDE)
    part_n[:, :, :WIDE] = dot_nn(scaled, wk[...]).astype(bf16).reshape(SEQS, PROPS, WIDE)
    part_n[:, :, WIDE:] = dot_nn(scaled, wv[...]).astype(bf16).reshape(SEQS, PROPS, WIDE)

    pl.semaphore_wait(barrier, NKV - 1 + tp_count - 1)

    def remote(src, dst, send, recv, where):
        return pltpu.make_async_remote_copy(
            src_ref=src, dst_ref=dst, send_sem=send, recv_sem=recv, device_id=where
        )

    def to_owners(body):
        @pl.loop(0, NZ)
        def _(i):
            z = lax.rem(my_z + far_first(i), NZ)
            for r in range(3):
                peer = owner_of(z, r)

                @pl.when(peer != me)
                def _():
                    body(3 * z + r, peer)

    def to_all(low, body):
        @pl.loop(0, NZ)
        def _(i):
            z = lax.rem(my_z + far_first(i), NZ)

            @pl.when(z >= low)
            def _():
                for k in range(NX):
                    x_at = lax.rem(my_x + (2, 1, 3, 0)[k], NX)
                    peer = z * NX + x_at

                    @pl.when(peer != me)
                    def _():
                        body(peer)

    def send_queries(b, peer):
        remote(part_q.at[b], got_q.at[me], send_sems.at[0], recv_sems.at[0], {"kv": peer}).start()
        remote(
            part_s.at[lax.div(b, 8)], got_s.at[me], send_sems.at[1], recv_sems.at[1], {"kv": peer}
        ).start()

    def send_new(b, peer):
        remote(part_n.at[b], got_n.at[me], send_sems.at[2], recv_sems.at[2], {"kv": peer}).start()

    to_owners(send_queries)
    to_owners(send_new)

    def all_arrived(ref, sem):
        most = ref.at[pl.ds(0, NKV - 1)]
        pltpu.make_async_copy(most, most, sem).wait()

    def own_inverse(sums, at):
        return lax.rsqrt(as_column(sums[0:1], at) / D + NORM_EPS)

    own_lane = lax.rem(own_b, 8) * PROPS

    @pl.when(owner)
    def _():
        got_q[me] = part_q[own_b]
        got_n[me] = part_n[own_b]
        got_s[me] = part_s[lax.div(own_b, 8)]
        all_arrived(got_s, recv_sems.at[1])
        all_arrived(got_q, recv_sems.at[0])
        sums = jnp.sum(got_s[...], axis=0)
        inverse = own_inverse(sums, own_lane)
        total = jnp.sum(got_q[...].astype(f32), axis=0)
        rounded = (inverse * total).astype(bf16).astype(f32)
        queries[own_b] = (rounded * HEAD**-0.5).astype(bf16)

        def send(peer):
            remote(
                queries.at[own_b],
                queries.at[own_b],
                send_sems.at[3],
                query_sems.at[own_b],
                {"kv": peer},
            ).start()

        to_all(0, send)

    for load in loads[6:9]:
        load.wait()
    positions = offset + iota((1, length), 1)

    @pl.loop(0, NZ)
    def _(i):
        z = lax.rem(my_z + near_first(i), NZ)
        for r in range(3):
            b = 3 * z + r
            peer = owner_of(z, r)

            @pl.when(peer != me)
            def _():
                mine = queries.at[b]
                pltpu.make_async_copy(mine, mine, query_sems.at[b]).wait()

        for r in range(3):
            b = 3 * z + r
            filled = prior_ref[b] + accepted_ref[b]
            gates_b = cum[b]
            last = jnp.sum(
                jnp.where(positions == filled - 1, gates_b, 0.0), axis=1, keepdims=True
            )
            bias = jnp.where(positions < filled, gates_b, MASKED)
            bias = jnp.concatenate(
                [jnp.broadcast_to(bias[h : h + 1], (PROPS, length)) for h in range(heads)], axis=0
            )
            scores = dot_nt(split_heads(queries[b].astype(f32)), keys[b]) - bias
            top = jnp.max(scores, axis=1, keepdims=True)
            weights = jnp.exp(scores - top)
            total = jnp.sum(weights, axis=1, keepdims=True)
            out_v[b] = join_heads(dot_nn(weights.astype(bf16), values[b])).astype(bf16)
            lane = iota((1, WIDE), 1)
            row = as_row(top, total)
            row = row + jnp.where(lane == 64, last[0:1], 0.0) + jnp.where(lane == 65, last[1:2], 0.0)
            out_s[b] = row

        for r in range(3):
            b = 3 * z + r
            peer = owner_of(z, r)

            @pl.when(peer != me)
            def _():
                remote(
                    out_s.at[b], got_m.at[me], send_sems.at[4], recv_sems.at[3], {"kv": peer}
                ).start()
                remote(
                    out_v.at[b], got_v.at[me], send_sems.at[5], recv_sems.at[4], {"kv": peer}
                ).start()

    @pl.when(owner)
    def _():
        got_v[me] = out_v[own_b]
        got_m[me] = out_s[own_b]

        all_arrived(got_n, recv_sems.at[2])
        sums = jnp.sum(got_s[...], axis=0)
        inverse = own_inverse(sums, own_lane)
        new = (inverse * jnp.sum(got_n[...].astype(f32), axis=0)).astype(bf16)
        own_new[...] = new

        def send(peer):
            remote(
                own_new, new_ref.at[own_b], send_sems.at[6], new_sems.at[own_b], {"kv": peer}
            ).start()

        to_all(FIRST_WRITER, send)

        seen = reach[...]
        seen_t = jnp.transpose(seen)[:PROPS]
        bias_rows = []
        for h in range(heads):
            logit = inverse * as_column(sums[h + 1 : h + 2], own_lane) + bias_ref[heads * tp + h]
            log_gate = jnp.minimum(logit, 0.0) - jnp.log1p(jnp.exp(-jnp.abs(logit)))
            tree_gate = jnp.sum(seen_t * log_gate, axis=0, keepdims=True)
            bias_rows.append(jnp.broadcast_to(tree_gate, (PROPS, WIDE)))
        rest = jnp.zeros((WIDE - PROPS, WIDE), bf16)
        new_keys = jnp.concatenate([new[:, :WIDE], rest], axis=0)
        new_values = jnp.concatenate([new[:, WIDE:], rest], axis=0)
        live = jnp.concatenate([seen[:PROPS], seen[:PROPS]], axis=0) > 0.5
        scores = dot_nt(split_heads(queries[own_b].astype(f32)), new_keys)
        scores = jnp.where(live, scores - jnp.concatenate(bias_rows, axis=0), -MASKED)
        top = jnp.max(scores, axis=1, keepdims=True)
        weights = jnp.where(live, jnp.exp(scores - top), 0.0)
        total = jnp.sum(weights, axis=1, keepdims=True)
        got_v[NKV] = join_heads(dot_nn(weights.astype(bf16), new_values)).astype(bf16)
        tree_row = as_row(top, total)

        all_arrived(got_m, recv_sems.at[3])
        lane = iota((1, WIDE), 1)
        stats = got_m[pl.ds(0, NKV)]
        ends = jnp.sum(stats, axis=0)
        last_0 = jnp.sum(jnp.where(lane == 64, ends, 0.0), axis=1, keepdims=True)
        last_1 = jnp.sum(jnp.where(lane == 65, ends, 0.0), axis=1, keepdims=True)
        shift = jnp.where(lane < PROPS, last_0, jnp.where(lane < 2 * PROPS, last_1, 0.0))
        got_m[NKV] = tree_row - shift
        stats = got_m[...]
        top = jnp.max(stats, axis=0, keepdims=True)
        held = lane.reshape(1, 1, WIDE) < 2 * PROPS
        factors = jnp.exp(jnp.where(held, stats - top, 0.0))
        sums_in = jnp.concatenate([stats[:, :, 32:], stats[:, :, :32]], axis=2)
        grand = jnp.sum(factors * sums_in, axis=0, keepdims=True)
        shares = factors / jnp.where(held, grand, 1.0)
        all_arrived(got_v, recv_sems.at[4])
        first = iota((PROPS, WIDE), 1) < HEAD
        result = jnp.zeros((PROPS, WIDE), f32)
        for s in range(NKV + 1):
            share = shares[s]
            pair = jnp.where(first, as_column(share, 0), as_column(share, PROPS))
            result = result + pair * got_v[s].astype(f32)
        attended[own_b] = result.astype(bf16)

        def send_rows(peer):
            remote(
                attended.at[own_b],
                attended.at[own_b],
                send_sems.at[7],
                att_sems.at[own_b],
                {"kv": peer},
            ).start()

        to_all(0, send_rows)

    loads[9].wait()
    per = NZ // tp_count

    @pl.loop(0, NZ)
    def _(i):
        z = lax.rem(my_z + near_first(i), NZ)
        for r in range(3):
            b = 3 * z + r
            peer = owner_of(z, r)

            @pl.when(peer != me)
            def _():
                mine = attended.at[b]
                pltpu.make_async_copy(mine, mine, att_sems.at[b]).wait()

        rows_in = attended[pl.ds(3 * z, 3)].reshape(3 * PROPS, WIDE)
        heads_out[z] = dot_nt(rows_in, wo[...]).astype(bf16)
        to, part = lax.div(z, per), lax.rem(z, per)

        @pl.when(to == tp)
        def _():
            heads_in[tp * per + part] = heads_out[z]

        @pl.when(to != tp)
        def _():
            remote(
                heads_out.at[z],
                heads_in.at[tp * per + part],
                send_sems.at[8],
                recv_sems.at[5],
                {"tp": to},
            ).start()

    def sent(ref, count, sem):
        some = ref.at[pl.ds(0, count)]
        pltpu.make_async_copy(some, some, sem).wait()

    if tp_count > 1:
        sent(heads_in, NZ - per, recv_sems.at[5])
    for part in range(per):
        total = heads_in[part].astype(f32)
        for s in range(1, tp_count):
            total = total + heads_in[s * per + part].astype(f32)
        mixed_ref[pl.ds(part * 3 * PROPS, 3 * PROPS), :] = total.astype(bf16)

    @pl.when(my_z >= FIRST_WRITER)
    def _():
        @pl.when(owner)
        def _():
            copy = pltpu.make_async_copy(own_new, new_ref.at[own_b], local_sems.at[10])
            copy.start()
            copy.wait()

        @pl.loop(0, NZ)
        def _(z):
            for r in range(3):

                @pl.when(owner_of(z, r) != me)
                def _():
                    there = new_ref.at[3 * z + r]
                    pltpu.make_async_copy(there, there, new_sems.at[3 * z + r]).wait()

    def sent_to_owners(count):
        sent(part_q, count, send_sems.at[0])
        sent(got_s, count, send_sems.at[1])
        sent(part_n, count, send_sems.at[2])
        sent(out_s, count, send_sems.at[4])
        sent(out_v, count, send_sems.at[5])

    @pl.when(owner)
    def _():
        sent_to_owners(SEQS - 1)
        sent(got_v, NKV - 1, send_sems.at[3])
        sent(got_v, NKV - 1, send_sems.at[7])
        writers = NKV - NX * FIRST_WRITER

        @pl.when(my_z >= FIRST_WRITER)
        def _():
            sent(part_n, writers - 1, send_sems.at[6])

        @pl.when(my_z < FIRST_WRITER)
        def _():
            sent(part_n, writers, send_sems.at[6])

    @pl.when(jnp.logical_not(owner))
    def _():
        sent_to_owners(SEQS)

    if tp_count > 1:
        sent(heads_out, NZ - per, send_sems.at[8])


def write_kernel(
    mixed_in, new_ref, prior_ref, accepted_ref, keys_hbm, values_hbm,
    mixed_out, keys_out, values_out,
    keys, values, sems_in, sems_out,
):
    me = lax.axis_index("kv")
    length = keys.shape[1]
    both = ((keys_hbm, keys, keys_out), (values_hbm, values, values_out))

    def copy_in(k, b):
        return pltpu.make_async_copy(both[k][0].at[b], both[k][1].at[b], sems_in.at[k, b])

    def copy_out(k, b):
        return pltpu.make_async_copy(both[k][1].at[b], both[k][2].at[b], sems_out.at[k, b])

    @pl.loop(0, SEQS)
    def _(b):
        for k in range(2):
            copy_in(k, b).start()

    mixed_out[...] = mixed_in[...]

    @pl.loop(0, SEQS)
    def _(b):
        start = prior_ref[b] + accepted_ref[b] - me * length
        touched = (start > -PROPS) & (start < length)
        for k in range(2):
            copy_in(k, b).wait()

        @pl.when(touched)
        def _():
            base = jnp.clip(lax.shift_right_arithmetic(start, 4), 0, length // PROPS - 2) * PROPS
            rows = pl.ds(pl.multiple_of(base, PROPS), 2 * PROPS)
            slot = iota((2 * PROPS, PROPS), 0) + (base - start)
            pick = jnp.where(slot == iota((2 * PROPS, PROPS), 1), 1.0, 0.0).astype(bf16)
            placed = dot_nn(pick, new_ref[b])
            at = iota((2 * PROPS, WIDE), 0) + (base - start)
            inside = (at >= 0) & (at < PROPS)
            for k in range(2):
                held = both[k][1]
                old = held[b, rows, :].astype(f32)
                fresh = placed[:, k * WIDE : (k + 1) * WIDE]
                held[b, rows, :] = jnp.where(inside, fresh, old).astype(bf16)

        for k in range(2):
            copy_out(k, b).start()

    @pl.loop(0, SEQS)
    def _(b):
        for k in range(2):
            copy_out(k, b).wait()


def shards(
    tokens, norm_gain, w_query, w_key, w_value, w_gate, gate_bias, w_out,
    keys_cache, values_cache, cum_gates, prior_len, accepted, parents,
):
    tp_count = lax.axis_size("tp")
    rows, width = tokens.shape
    columns = w_out.shape[1]
    length = keys_cache.shape[1]
    any_ = pl.BlockSpec(memory_space=pl.ANY)
    smem = pl.BlockSpec(memory_space=pltpu.SMEM)
    vmem = pl.BlockSpec(memory_space=pltpu.VMEM)
    out_rows = rows // tp_count
    dma = pltpu.SemaphoreType.DMA
    mixed, new = pl.pallas_call(
        functools.partial(step_kernel, tp_count),
        out_shape=(
            jax.ShapeDtypeStruct((out_rows, columns), bf16),
            jax.ShapeDtypeStruct((SEQS, PROPS, 2 * WIDE), bf16),
        ),
        in_specs=[any_] * 10 + [smem] * 4,
        out_specs=(vmem, any_),
        scratch_shapes=[
            pltpu.VMEM((width, rows), bf16),
            pltpu.VMEM((1, width), f32),
            pltpu.VMEM((width, WIDE), bf16),
            pltpu.VMEM((width, WIDE), bf16),
            pltpu.VMEM((width, WIDE), bf16),
            pltpu.VMEM((w_gate.shape[1], WIDE), bf16),
            pltpu.VMEM((columns, WIDE), bf16),
            pltpu.VMEM(keys_cache.shape, bf16),
            pltpu.VMEM(values_cache.shape, bf16),
            pltpu.VMEM(cum_gates.shape, f32),
            pltpu.VMEM((SEQS, PROPS, WIDE), bf16),
            pltpu.VMEM((SEQS, PROPS, 2 * WIDE), bf16),
            pltpu.VMEM((3, 4, WIDE), f32),
            pltpu.VMEM((NKV, PROPS, WIDE), bf16),
            pltpu.VMEM((NKV, PROPS, 2 * WIDE), bf16),
            pltpu.VMEM((NKV, 4, WIDE), f32),
            pltpu.VMEM((SEQS, PROPS, WIDE), bf16),
            pltpu.VMEM((PROPS, 2 * WIDE), bf16),
            pltpu.VMEM((SEQS, PROPS, WIDE), bf16),
            pltpu.VMEM((SEQS, 1, WIDE), f32),
            pltpu.VMEM((NKV + 1, PROPS, WIDE), bf16),
            pltpu.VMEM((NKV + 1, 1, WIDE), f32),
            pltpu.VMEM((SEQS, PROPS, WIDE), bf16),
            pltpu.VMEM((WIDE, WIDE), f32),
            pltpu.VMEM((NZ, 3 * PROPS, columns), bf16),
            pltpu.VMEM((NZ, 3 * PROPS, columns), bf16),
            dma((11,)),
            dma((9,)),
            dma((6,)),
            dma((SEQS,)),
            dma((SEQS,)),
            dma((SEQS,)),
        ],
        compiler_params=pltpu.CompilerParams(collective_id=0, has_side_effects=True),
        name="tree_step",
    )(
        tokens.T, norm_gain.reshape(1, width), w_query, w_key, w_value, w_gate.T, w_out.T,
        keys_cache, values_cache, cum_gates, gate_bias, prior_len, accepted, parents.T,
    )
    return pl.pallas_call(
        write_kernel,
        out_shape=(
            jax.ShapeDtypeStruct((out_rows, columns), bf16),
            jax.ShapeDtypeStruct(keys_cache.shape, bf16),
            jax.ShapeDtypeStruct(values_cache.shape, bf16),
        ),
        in_specs=[vmem, vmem, smem, smem, any_, any_],
        out_specs=(vmem, any_, any_),
        scratch_shapes=[
            pltpu.VMEM(keys_cache.shape, bf16),
            pltpu.VMEM(values_cache.shape, bf16),
            dma((2, SEQS)),
            dma((2, SEQS)),
        ],
        name="cache_write",
    )(mixed, new, prior_len, accepted, keys_cache, values_cache)


def solution(mesh):
    in_specs = (
        P(None, "kv"),
        P("kv"),
        P("kv", "tp"),
        P("kv", "tp"),
        P("kv", "tp"),
        P(),
        P(),
        P("tp", "kv"),
        P(None, "kv", "tp"),
        P(None, "kv", "tp"),
        P(None, "tp", "kv"),
        P(),
        P(),
        P(),
    )
    out_specs = (P("tp", "kv"), P(None, "kv", "tp"), P(None, "kv", "tp"))
    return jax.shard_map(
        shards, mesh=mesh, in_specs=in_specs, out_specs=out_specs, check_vma=False
    )
```

```python
import functools

import jax
import jax.numpy as jnp
from jax import lax
from jax.experimental import pallas as pl
from jax.experimental.pallas import tpu as pltpu
from jax.sharding import PartitionSpec as P

D = 2048
HEAD = 64
PROPS = 16
SEQS = 24
NZ, NX = 8, 4
NKV = NZ * NX
WIDE = 128
MASKED = 1e30
NORM_EPS = 1e-06
FIRST_WRITER = 4

f32, bf16 = jnp.float32, jnp.bfloat16


def iota(shape, dim):
    return lax.broadcasted_iota(jnp.int32, shape, dim)


def dot_nt(a, b):
    return lax.dot_general(a, b, (((1,), (1,)), ((), ())), preferred_element_type=f32)


def dot_nn(a, b):
    return lax.dot_general(a, b, (((1,), (0,)), ((), ())), preferred_element_type=f32)


def far_first(i):
    return 4 + (1 - 2 * lax.rem(i, 2)) * lax.div(i + 1, 2)


def near_first(i):
    odd = lax.rem(i, 2)
    return odd * lax.div(i + 1, 2) + (1 - odd) * lax.rem(NZ - lax.div(i, 2), NZ)


def owner_of(z, r):
    return z * NX + lax.rem(z + 1 + r, NX)


def split_heads(rows):
    lane = iota((2 * PROPS, WIDE), 1)
    sub = iota((2 * PROPS, WIDE), 0)
    both = jnp.concatenate([rows, rows], axis=0)
    return jnp.where((lane < HEAD) == (sub < PROPS), both, 0.0).astype(bf16)


def join_heads(rows):
    lane = iota((PROPS, WIDE), 1)
    return jnp.where(lane < HEAD, rows[:PROPS], rows[PROPS:])


def as_row(tops, sums):
    lane = iota((2 * PROPS, WIDE), 1)
    sub = iota((2 * PROPS, WIDE), 0)
    spread = jnp.where(lane == sub, tops, jnp.where(lane == sub + 2 * PROPS, sums, 0.0))
    return jnp.sum(spread, axis=0, keepdims=True)


def as_column(row, start):
    lane = iota((PROPS, WIDE), 1)
    sub = iota((PROPS, WIDE), 0)
    return jnp.sum(jnp.where(lane == sub + start, row, 0.0), axis=1, keepdims=True)


def step_kernel(
    tp_count,
    tok_hbm,
    gain_hbm,
    wq_hbm,
    wk_hbm,
    wv_hbm,
    wg_hbm,
    wo_hbm,
    keys_hbm,
    values_hbm,
    cum_hbm,
    bias_hbm,
    prior_hbm,
    accepted_hbm,
    parents_hbm,
    mixed_ref,
    new_ref,
    keys,
    values,
    bias_ref,
    prior_ref,
    accepted_ref,
    parents_ref,
    tok,
    gain,
    wq,
    wk,
    wv,
    wg,
    wo,
    keys_t,
    cum,
    part_q,
    part_n,
    part_s,
    got_q,
    got_n,
    got_s,
    queries,
    own_new,
    out_v,
    out_s,
    got_v,
    got_m,
    own_rows,
    got_rows,
    reach,
    local_sems,
    send_sems,
    recv_sems,
    query_sems,
    new_sems,
    planes_in,
):
    me = lax.axis_index("kv")
    tp = lax.axis_index("tp")
    my_z, my_x = lax.div(me, NX), lax.rem(me, NX)
    my_r = lax.rem(my_x - my_z - 1 + 2 * NX * NZ, NX)
    owner = my_r < 3
    own_b = lax.min(my_z + NZ * my_r, SEQS - 1)
    per = SEQS // tp_count
    own_to = lax.div(own_b, per)
    length = keys.shape[1]
    offset = me * length
    heads = 2

    barrier = pltpu.get_barrier_semaphore()

    @pl.loop(0, NKV - 1)
    def _(i):
        pl.semaphore_signal(barrier, inc=1, device_id={"kv": lax.rem(me + i + 1, NKV)})

    @pl.loop(0, tp_count - 1)
    def _(i):
        pl.semaphore_signal(barrier, inc=1, device_id={"tp": lax.rem(tp + i + 1, tp_count)})

    gate_block = pl.multiple_of(lax.div(me, 2) * WIDE, WIDE)
    pairs = (
        (parents_hbm, parents_ref),
        (bias_hbm, bias_ref),
        (prior_hbm, prior_ref),
        (accepted_hbm, accepted_ref),
        (tok_hbm, tok),
        (gain_hbm, gain),
        (wg_hbm.at[:, pl.ds(gate_block, WIDE)], wg),
        (wq_hbm, wq),
        (wk_hbm, wk),
        (wv_hbm, wv),
        (cum_hbm, cum),
        (keys_hbm, keys),
        (values_hbm, values),
        (wo_hbm, wo.at[tp]),
    )
    loads = [pltpu.make_async_copy(a, b, local_sems.at[i]) for i, (a, b) in enumerate(pairs)]
    for load in loads:
        load.start()

    loads[0].wait()

    @pl.when(owner)
    def _():
        lane = iota((PROPS, WIDE), 1)
        sub = iota((PROPS, WIDE), 0)
        parent = jnp.full((PROPS, WIDE), -1, jnp.int32)
        for j in range(PROPS):
            parent = jnp.where(sub == j, parents_ref[j, own_b], parent)
        seen = jnp.where((lane == sub) | (lane == parent), 1.0, 0.0)
        rest = jnp.zeros((WIDE - PROPS, WIDE), f32)
        for _ in range(4):
            square = jnp.concatenate([seen, rest], axis=0).astype(bf16)
            seen = jnp.minimum(dot_nn(seen.astype(bf16), square), 1.0)
        reach[...] = jnp.concatenate([seen, rest], axis=0)

    with jax.named_scope("wait_inputs"):
        for load in loads[4:10]:
            load.wait()
    x = tok[...].astype(f32)
    width = x.shape[0]
    eye = iota((width, width), 0) == iota((width, width), 1)
    gain_col = jnp.sum(jnp.where(eye, gain[...], 0.0), axis=1, keepdims=True)
    square_row = jnp.sum(x * x, axis=0, keepdims=True)
    scaled_t = x * gain_col
    scaled = jnp.transpose(scaled_t).astype(bf16)
    gate_w = wg[...].astype(f32)
    gate_w = jnp.where(lax.rem(me, 2) == 0, gate_w[:, :width], gate_w[:, width:]).astype(bf16)
    gates = dot_nn(gate_w, scaled_t.astype(bf16))
    gate_row = iota(gates.shape, 0)
    rows = [square_row] + [
        jnp.sum(jnp.where(gate_row == heads * tp + h, gates, 0.0), axis=0, keepdims=True)
        for h in range(heads)
    ]
    sub, lane = iota((8, WIDE), 0), iota((8, WIDE), 1)
    for j in range(3):
        tile = jnp.zeros((8, WIDE), f32)
        for k, row in enumerate(rows):
            part = row[:, j * WIDE : (j + 1) * WIDE]
            part = pltpu.roll(jnp.broadcast_to(part, (8, WIDE)), k * PROPS, 1)
            tile = jnp.where(sub == k, part, tile)
        for c in range(8):
            moved = pltpu.roll(tile, (WIDE - c * PROPS) % WIDE, 1)
            moved = jnp.where(lax.shift_right_logical(lane, 4) == sub, moved, 0.0)
            part_s[8 * j + c] = jnp.sum(moved, axis=0, keepdims=True)
    part_q[...] = dot_nn(scaled, wq[...]).astype(bf16).reshape(SEQS, PROPS, WIDE)
    part_n[:, :, :WIDE] = dot_nn(scaled, wk[...]).astype(bf16).reshape(SEQS, PROPS, WIDE)
    part_n[:, :, WIDE:] = dot_nn(scaled, wv[...]).astype(bf16).reshape(SEQS, PROPS, WIDE)

    with jax.named_scope("barrier"):
        pl.semaphore_wait(barrier, NKV - 1 + tp_count - 1)

    def remote(src, dst, send, recv, where):
        return pltpu.make_async_remote_copy(
            src_ref=src, dst_ref=dst, send_sem=send, recv_sem=recv, device_id=where
        )

    def to_owners(body):
        @pl.loop(0, NZ)
        def _(i):
            z = lax.rem(my_z + far_first(i), NZ)
            for r in range(3):
                peer = owner_of(z, r)

                @pl.when(peer != me)
                def _():
                    body(z + NZ * r, peer)

    def to_everyone(low, body):
        @pl.loop(0, NZ)
        def _(i):
            z = lax.rem(my_z + far_first(i), NZ)

            @pl.when(z >= low)
            def _():
                for k in range(NX):
                    body(z * NX + lax.rem(my_x + (2, 1, 3, 0)[k], NX))

    def to_all(low, body):
        def other(peer):
            @pl.when(peer != me)
            def _():
                body(peer)

        to_everyone(low, other)

    def send_queries(b, peer):
        remote(part_q.at[b], got_q.at[me], send_sems.at[0], recv_sems.at[0], {"kv": peer}).start()
        remote(part_s.at[b], got_s.at[me], send_sems.at[1], recv_sems.at[1], {"kv": peer}).start()

    def send_new(b, peer):
        remote(part_n.at[b], got_n.at[me], send_sems.at[2], recv_sems.at[2], {"kv": peer}).start()

    with jax.named_scope("send_parts"):
        to_owners(send_queries)

    loads[13].wait()

    @pl.loop(0, tp_count - 1)
    def _(i):
        there = {"tp": lax.rem(tp + i + 1, tp_count)}
        pl.semaphore_signal(planes_in, inc=1, device_id=there)
        remote(wo.at[tp], wo.at[tp], send_sems.at[8], recv_sems.at[5], there).start()

    with jax.named_scope("wait_cache"):
        for load in (loads[1], loads[2], loads[3], loads[10], loads[11]):
            load.wait()
    positions = offset + iota((1, length), 1)

    with jax.named_scope("prepare"):

        @pl.loop(0, SEQS)
        def _(b):
            filled = prior_ref[b] + accepted_ref[b]
            gates_b = cum[b]
            last = jnp.sum(
                jnp.where(positions == filled - 1, gates_b, 0.0), axis=1, keepdims=True
            )
            cum[b] = jnp.where(positions < filled, gates_b, MASKED)
            lane = iota((1, WIDE), 1)
            row = jnp.where(lane == 64, last[0:1], 0.0) + jnp.where(lane == 65, last[1:2], 0.0)
            out_s[b] = row
            keys_t[b] = jnp.transpose(keys[b])

    def all_arrived(ref, sem):
        most = ref.at[pl.ds(0, NKV - 1)]
        pltpu.make_async_copy(most, most, sem).wait()

    def own_inverse(sums):
        return lax.rsqrt(as_column(sums, 0) / D + NORM_EPS)

    @pl.when(owner)
    def _():
        got_q[me] = part_q[own_b]
        got_n[me] = part_n[own_b]
        got_s[me] = part_s[own_b]
        with jax.named_scope("wait_parts"):
            all_arrived(got_s, recv_sems.at[1])
            all_arrived(got_q, recv_sems.at[0])
        sums = jnp.sum(got_s[...], axis=0)
        inverse = own_inverse(sums)
        total = jnp.sum(got_q[...].astype(f32), axis=0)
        rounded = (inverse * total).astype(bf16).astype(f32)
        queries[own_b] = (rounded * HEAD**-0.5).astype(bf16)

        def send(peer):
            remote(
                queries.at[own_b],
                queries.at[own_b],
                send_sems.at[3],
                query_sems.at[own_b],
                {"kv": peer},
            ).start()

        with jax.named_scope("send_queries"):
            to_all(0, send)

    with jax.named_scope("send_new"):
        to_owners(send_new)

    with jax.named_scope("wait_cache"):
        loads[12].wait()

    @pl.loop(0, NZ)
    def _(i):
        z = lax.rem(my_z + near_first(i), NZ)
        for r in range(3):
            b = z + NZ * r
            peer = owner_of(z, r)

            @pl.when(peer != me)
            def _():
                with jax.named_scope("wait_query"):
                    mine = queries.at[b]
                    pltpu.make_async_copy(mine, mine, query_sems.at[b]).wait()

        group = range(3)
        scores = []
        for r in group:
            bias = cum[z + NZ * r]
            bias = jnp.concatenate(
                [jnp.broadcast_to(bias[h : h + 1], (PROPS, length)) for h in range(heads)], axis=0
            )
            query = split_heads(queries[z + NZ * r].astype(f32))
            scores.append(dot_nn(query, keys_t[z + NZ * r]) - bias)
        tops = [jnp.max(scores[r], axis=1, keepdims=True) for r in group]
        weights = [jnp.exp(scores[r] - tops[r]) for r in group]
        totals = [jnp.sum(weights[r], axis=1, keepdims=True) for r in group]
        blocks = [dot_nn(weights[r].astype(bf16), values[z + NZ * r]) for r in group]
        for r in group:
            out_s[z + NZ * r] = out_s[z + NZ * r] + as_row(tops[r], totals[r])
            out_v[z + NZ * r] = join_heads(blocks[r]).astype(bf16)

        for r in range(3):
            b = z + NZ * r
            peer = owner_of(z, r)

            @pl.when(peer != me)
            def _():
                remote(
                    out_s.at[b], got_m.at[me], send_sems.at[4], recv_sems.at[3], {"kv": peer}
                ).start()
                remote(
                    out_v.at[b], got_v.at[me], send_sems.at[5], recv_sems.at[4], {"kv": peer}
                ).start()

    @pl.when(owner)
    def _():
        got_v[me] = out_v[own_b]
        got_m[me] = out_s[own_b]

        with jax.named_scope("wait_new"):
            all_arrived(got_n, recv_sems.at[2])
        sums = jnp.sum(got_s[...], axis=0)
        inverse = own_inverse(sums)
        new = (inverse * jnp.sum(got_n[...].astype(f32), axis=0)).astype(bf16)
        own_new[...] = new

        def send(peer):
            remote(
                own_new, new_ref.at[own_b], send_sems.at[6], new_sems.at[own_b], {"kv": peer}
            ).start()

        to_all(FIRST_WRITER, send)

        seen = reach[...]
        seen_t = jnp.transpose(seen)[:PROPS]
        bias_rows = []
        for h in range(heads):
            logit = inverse * as_column(sums, PROPS * (h + 1)) + bias_ref[heads * tp + h]
            log_gate = jnp.minimum(logit, 0.0) - jnp.log1p(jnp.exp(-jnp.abs(logit)))
            tree_gate = jnp.sum(seen_t * log_gate, axis=0, keepdims=True)
            bias_rows.append(jnp.broadcast_to(tree_gate, (PROPS, WIDE)))
        rest = jnp.zeros((WIDE - PROPS, WIDE), bf16)
        new_keys = jnp.concatenate([new[:, :WIDE], rest], axis=0)
        new_values = jnp.concatenate([new[:, WIDE:], rest], axis=0)
        live = jnp.concatenate([seen[:PROPS], seen[:PROPS]], axis=0) > 0.5
        scores = dot_nt(split_heads(queries[own_b].astype(f32)), new_keys)
        scores = jnp.where(live, scores - jnp.concatenate(bias_rows, axis=0), -MASKED)
        top = jnp.max(scores, axis=1, keepdims=True)
        weights = jnp.where(live, jnp.exp(scores - top), 0.0)
        total = jnp.sum(weights, axis=1, keepdims=True)
        got_v[NKV] = join_heads(dot_nn(weights.astype(bf16), new_values)).astype(bf16)
        tree_row = as_row(top, total)

        with jax.named_scope("wait_stats"):
            all_arrived(got_m, recv_sems.at[3])
        lane = iota((1, WIDE), 1)
        stats = got_m[pl.ds(0, NKV)]
        ends = jnp.sum(stats, axis=0)
        last_0 = jnp.sum(jnp.where(lane == 64, ends, 0.0), axis=1, keepdims=True)
        last_1 = jnp.sum(jnp.where(lane == 65, ends, 0.0), axis=1, keepdims=True)
        shift = jnp.where(lane < PROPS, last_0, jnp.where(lane < 2 * PROPS, last_1, 0.0))
        got_m[NKV] = tree_row - shift
        stats = got_m[...]
        top = jnp.max(stats, axis=0, keepdims=True)
        held = lane.reshape(1, 1, WIDE) < 2 * PROPS
        factors = jnp.exp(jnp.where(held, stats - top, 0.0))
        sums_in = jnp.concatenate([stats[:, :, 32:], stats[:, :, :32]], axis=2)
        grand = jnp.sum(factors * sums_in, axis=0, keepdims=True)
        shares = factors / jnp.where(held, grand, 1.0)
        with jax.named_scope("wait_blocks"):
            all_arrived(got_v, recv_sems.at[4])
        first = iota((PROPS, WIDE), 1) < HEAD
        result = jnp.zeros((PROPS, WIDE), f32)
        for s in range(NKV + 1):
            share = shares[s]
            pair = jnp.where(first, as_column(share, 0), as_column(share, PROPS))
            result = result + pair * got_v[s].astype(f32)
        own_rows[...] = result.astype(bf16)
        slot = lax.rem(own_b, per)

        if tp_count > 1:
            pl.semaphore_wait(planes_in, tp_count - 1)

        def send_rows(peer):
            @pl.when(jnp.logical_or(peer != me, own_to != tp))
            def _():
                remote(
                    own_rows,
                    got_rows.at[tp, slot],
                    send_sems.at[7],
                    recv_sems.at[6],
                    {"kv": peer, "tp": own_to},
                ).start()

        with jax.named_scope("send_rows"):
            to_everyone(0, send_rows)

        @pl.when(own_to == tp)
        def _():
            got_rows[tp, slot] = own_rows[...]

    def arrived(ref, count, sem):
        some = ref.at[pl.ds(0, count)]
        pltpu.make_async_copy(some, some, sem).wait()

    sent = arrived
    if tp_count > 1:
        arrived(wo, tp_count - 1, recv_sems.at[5])

    with jax.named_scope("wait_rows"):
        mine_too = jnp.logical_and(owner, own_to == tp)

        @pl.when(mine_too)
        def _():
            arrived(got_v, tp_count * per - 1, recv_sems.at[6])

        @pl.when(jnp.logical_not(mine_too))
        def _():
            arrived(got_v, tp_count * per, recv_sems.at[6])

    total = jnp.zeros((per * PROPS, wo.shape[1]), f32)
    for s in range(tp_count):
        rows_in = got_rows[s].reshape(per * PROPS, WIDE)
        total = total + dot_nt(rows_in, wo[s]).astype(bf16).astype(f32)
    mixed_ref[...] = total.astype(bf16)

    @pl.when(my_z >= FIRST_WRITER)
    def _():
        @pl.when(owner)
        def _():
            copy = pltpu.make_async_copy(own_new, new_ref.at[own_b], local_sems.at[14])
            copy.start()
            copy.wait()

        @pl.loop(0, NZ)
        def _(z):
            for r in range(3):

                @pl.when(owner_of(z, r) != me)
                @jax.named_scope("wait_fresh")
                def _():
                    there = new_ref.at[z + NZ * r]
                    pltpu.make_async_copy(there, there, new_sems.at[z + NZ * r]).wait()

    def sent_to_owners(count):
        sent(part_q, count, send_sems.at[0])
        sent(got_s, count, send_sems.at[1])
        sent(part_n, count, send_sems.at[2])
        sent(out_s, count, send_sems.at[4])
        sent(out_v, count, send_sems.at[5])

    @pl.when(owner)
    def _():
        sent_to_owners(SEQS - 1)
        sent(got_v, NKV - 1, send_sems.at[3])

        @pl.when(own_to == tp)
        def _():
            sent(got_v, NKV - 1, send_sems.at[7])

        @pl.when(own_to != tp)
        def _():
            sent(got_v, NKV, send_sems.at[7])

        writers = NKV - NX * FIRST_WRITER

        @pl.when(my_z >= FIRST_WRITER)
        def _():
            sent(part_n, writers - 1, send_sems.at[6])

        @pl.when(my_z < FIRST_WRITER)
        def _():
            sent(part_n, writers, send_sems.at[6])

    @pl.when(jnp.logical_not(owner))
    def _():
        sent_to_owners(SEQS)

    if tp_count > 1:

        @pl.when(jnp.logical_not(owner))
        def _():
            pl.semaphore_wait(planes_in, tp_count - 1)

        sent(wo, tp_count - 1, send_sems.at[8])


def write_kernel(
    mixed_in, new_ref, prior_ref, accepted_ref, keys, values,
    mixed_out, keys_out, values_out, sems_out, sem_mixed,
):
    me = lax.axis_index("kv")
    length = keys.shape[1]
    both = ((keys, keys_out), (values, values_out))

    def copy_out(k, b):
        return pltpu.make_async_copy(both[k][0].at[b], both[k][1].at[b], sems_out.at[k, b])

    mixed = pltpu.make_async_copy(mixed_in, mixed_out, sem_mixed)
    mixed.start()

    @pl.loop(0, SEQS)
    def _(b):
        start = prior_ref[b] + accepted_ref[b] - me * length

        @pl.when((start > -PROPS) & (start < length))
        def _():
            base = jnp.clip(lax.shift_right_arithmetic(start, 4), 0, length // PROPS - 2) * PROPS
            rows = pl.ds(pl.multiple_of(base, PROPS), 2 * PROPS)
            slot = iota((2 * PROPS, PROPS), 0) + (base - start)
            pick = jnp.where(slot == iota((2 * PROPS, PROPS), 1), 1.0, 0.0).astype(bf16)
            placed = dot_nn(pick, new_ref[b])
            at = iota((2 * PROPS, WIDE), 0) + (base - start)
            inside = (at >= 0) & (at < PROPS)
            for k in range(2):
                held = both[k][0]
                old = held[b, rows, :].astype(f32)
                fresh = placed[:, k * WIDE : (k + 1) * WIDE]
                held[b, rows, :] = jnp.where(inside, fresh, old).astype(bf16)

        for k in range(2):
            copy_out(k, b).start()

    @pl.loop(0, SEQS)
    def _(b):
        for k in range(2):
            copy_out(k, b).wait()

    mixed.wait()


def on_chip(shape, dtype):
    return pltpu.VMEM(shape, dtype)


def shards(
    tokens, norm_gain, w_query, w_key, w_value, w_gate, gate_bias, w_out,
    keys_cache, values_cache, cum_gates, prior_len, accepted, parents,
):
    tp_count = lax.axis_size("tp")
    rows, width = tokens.shape
    columns = w_out.shape[1]
    length = keys_cache.shape[1]
    any_ = pl.BlockSpec(memory_space=pl.ANY)
    smem = pl.BlockSpec(memory_space=pltpu.SMEM)
    vmem = pl.BlockSpec(memory_space=pltpu.VMEM)
    out_rows = rows // tp_count
    dma = pltpu.SemaphoreType.DMA
    mixed, new, keys_held, values_held = pl.pallas_call(
        functools.partial(step_kernel, tp_count),
        out_shape=(
            on_chip((out_rows, columns), bf16),
            on_chip((SEQS, PROPS, 2 * WIDE), bf16),
            on_chip(keys_cache.shape, bf16),
            on_chip(values_cache.shape, bf16),
        ),
        in_specs=[pl.BlockSpec(memory_space=pltpu.HBM)] * 14,
        out_specs=(vmem, vmem, vmem, vmem),
        scratch_shapes=[
            pltpu.SMEM(gate_bias.shape, f32),
            pltpu.SMEM(prior_len.shape, jnp.int32),
            pltpu.SMEM(accepted.shape, jnp.int32),
            pltpu.SMEM(parents.shape[::-1], jnp.int32),
            pltpu.VMEM((width, rows), bf16),
            pltpu.VMEM((1, width), f32),
            pltpu.VMEM((width, WIDE), bf16),
            pltpu.VMEM((width, WIDE), bf16),
            pltpu.VMEM((width, WIDE), bf16),
            pltpu.VMEM((w_gate.shape[1], WIDE), bf16),
            pltpu.VMEM((tp_count, columns, WIDE), bf16),
            pltpu.VMEM((SEQS, WIDE, length), bf16),
            pltpu.VMEM(cum_gates.shape, f32),
            pltpu.VMEM((SEQS, PROPS, WIDE), bf16),
            pltpu.VMEM((SEQS, PROPS, 2 * WIDE), bf16),
            pltpu.VMEM((SEQS, 1, WIDE), f32),
            pltpu.VMEM((NKV, PROPS, WIDE), bf16),
            pltpu.VMEM((NKV, PROPS, 2 * WIDE), bf16),
            pltpu.VMEM((NKV, 1, WIDE), f32),
            pltpu.VMEM((SEQS, PROPS, WIDE), bf16),
            pltpu.VMEM((PROPS, 2 * WIDE), bf16),
            pltpu.VMEM((SEQS, PROPS, WIDE), bf16),
            pltpu.VMEM((SEQS, 1, WIDE), f32),
            pltpu.VMEM((NKV + 1, PROPS, WIDE), bf16),
            pltpu.VMEM((NKV + 1, 1, WIDE), f32),
            pltpu.VMEM((PROPS, WIDE), bf16),
            pltpu.VMEM((tp_count, SEQS // tp_count, PROPS, WIDE), bf16),
            pltpu.VMEM((WIDE, WIDE), f32),
            dma((15,)),
            dma((9,)),
            dma((7,)),
            dma((SEQS,)),
            dma((SEQS,)),
            pltpu.SemaphoreType.REGULAR,
        ],
        compiler_params=pltpu.CompilerParams(
            collective_id=0, has_side_effects=True, vmem_limit_bytes=24 << 20
        ),
        name="tree_step",
    )(
        *(
            pltpu.with_memory_space_constraint(x, pltpu.HBM)
            for x in (
                tokens.T, norm_gain.reshape(1, width), w_query, w_key, w_value, w_gate.T, w_out.T,
                keys_cache, values_cache, cum_gates, gate_bias, prior_len, accepted, parents.T,
            )
        )
    )

    def held(x):
        return pltpu.with_memory_space_constraint(x, pltpu.VMEM)

    return pl.pallas_call(
        write_kernel,
        out_shape=(
            jax.ShapeDtypeStruct((out_rows, columns), bf16),
            jax.ShapeDtypeStruct(keys_cache.shape, bf16),
            jax.ShapeDtypeStruct(values_cache.shape, bf16),
        ),
        in_specs=[vmem, vmem, smem, smem, vmem, vmem],
        out_specs=(any_, any_, any_),
        scratch_shapes=[dma((2, SEQS)), dma],
        compiler_params=pltpu.CompilerParams(vmem_limit_bytes=8 << 20),
        name="cache_write",
    )(held(mixed), held(new), prior_len, accepted, held(keys_held), held(values_held))


def solution(mesh):
    in_specs = (
        P(None, "kv"),
        P("kv"),
        P("kv", "tp"),
        P("kv", "tp"),
        P("kv", "tp"),
        P(),
        P(),
        P("tp", "kv"),
        P(None, "kv", "tp"),
        P(None, "kv", "tp"),
        P(None, "tp", "kv"),
        P(),
        P(),
        P(),
    )
    out_specs = (P("tp", "kv"), P(None, "kv", "tp"), P(None, "kv", "tp"))
    return jax.shard_map(
        shards, mesh=mesh, in_specs=in_specs, out_specs=out_specs, check_vma=False
    )
```

```python
import functools

import jax
import jax.numpy as jnp
from jax import lax
from jax.experimental import pallas as pl
from jax.experimental.pallas import tpu as pltpu
from jax.sharding import PartitionSpec as P

D = 2048
HEAD = 64
PROPS = 16
SEQS = 24
NZ, NX = 8, 4
NKV = NZ * NX
WIDE = 128
MASKED = 1e30
NORM_EPS = 1e-06
FIRST_WRITER = 4

f32, bf16 = jnp.float32, jnp.bfloat16


def iota(shape, dim):
    return lax.broadcasted_iota(jnp.int32, shape, dim)


def dot_nt(a, b):
    return lax.dot_general(a, b, (((1,), (1,)), ((), ())), preferred_element_type=f32)


def dot_nn(a, b):
    return lax.dot_general(a, b, (((1,), (0,)), ((), ())), preferred_element_type=f32)


def far_first(i):
    return 4 + (1 - 2 * lax.rem(i, 2)) * lax.div(i + 1, 2)


def near_first(i):
    odd = lax.rem(i, 2)
    return odd * lax.div(i + 1, 2) + (1 - odd) * lax.rem(NZ - lax.div(i, 2), NZ)


def owner_of(z, r):
    return z * NX + lax.rem(z + 1 + r, NX)


def split_heads(rows):
    lane = iota((2 * PROPS, WIDE), 1)
    sub = iota((2 * PROPS, WIDE), 0)
    both = jnp.concatenate([rows, rows], axis=0)
    return jnp.where((lane < HEAD) == (sub < PROPS), both, 0.0).astype(bf16)


def join_heads(rows):
    lane = iota((PROPS, WIDE), 1)
    return jnp.where(lane < HEAD, rows[:PROPS], rows[PROPS:])


def as_row(tops, sums):
    lane = iota((2 * PROPS, WIDE), 1)
    sub = iota((2 * PROPS, WIDE), 0)
    spread = jnp.where(lane == sub, tops, jnp.where(lane == sub + 2 * PROPS, sums, 0.0))
    return jnp.sum(spread, axis=0, keepdims=True)


def as_column(row, start):
    lane = iota((PROPS, WIDE), 1)
    sub = iota((PROPS, WIDE), 0)
    return jnp.sum(jnp.where(lane == sub + start, row, 0.0), axis=1, keepdims=True)


def step_kernel(
    tp_count,
    tok_hbm,
    gain_hbm,
    wq_hbm,
    wk_hbm,
    wv_hbm,
    wg_hbm,
    wo_hbm,
    keys_hbm,
    values_hbm,
    cum_hbm,
    bias_hbm,
    prior_hbm,
    accepted_hbm,
    parents_hbm,
    mixed_ref,
    new_ref,
    keys,
    values,
    bias_ref,
    prior_ref,
    accepted_ref,
    parents_ref,
    tok,
    gain,
    wq,
    wk,
    wv,
    wg,
    wo,
    keys_t,
    cum,
    part_q,
    part_n,
    part_s,
    got_q,
    got_x,
    sum_x,
    got_n,
    got_s,
    queries,
    own_new,
    out_v,
    out_s,
    got_v,
    got_m,
    own_rows,
    got_rows,
    reach,
    local_sems,
    send_sems,
    recv_sems,
    query_sems,
    row_sems,
    planes_in,
):
    me = lax.axis_index("kv")
    tp = lax.axis_index("tp")
    my_z, my_x = lax.div(me, NX), lax.rem(me, NX)
    my_r = lax.rem(my_x - my_z - 1 + 2 * NX * NZ, NX)
    owner = my_r < 3
    own_b = lax.min(my_z + NZ * my_r, SEQS - 1)
    per = SEQS // tp_count
    own_to = lax.div(own_b, per)
    length = keys.shape[1]
    offset = me * length
    heads = 2

    barrier = pltpu.get_barrier_semaphore()

    @pl.loop(0, NZ)
    def _(i):
        z = lax.rem(my_z + far_first(i), NZ)
        for k in range(NX):
            peer = z * NX + lax.rem(my_x + (2, 1, 3, 0)[k], NX)

            @pl.when(peer != me)
            def _():
                pl.semaphore_signal(barrier, inc=1, device_id={"kv": peer})

    @pl.loop(0, tp_count - 1)
    def _(i):
        pl.semaphore_signal(barrier, inc=1, device_id={"tp": lax.rem(tp + i + 1, tp_count)})

    gate_block = pl.multiple_of(lax.div(me, 2) * WIDE, WIDE)
    pairs = (
        (parents_hbm, parents_ref),
        (bias_hbm, bias_ref),
        (prior_hbm, prior_ref),
        (accepted_hbm, accepted_ref),
        (tok_hbm, tok),
        (gain_hbm, gain),
        (wg_hbm.at[:, pl.ds(gate_block, WIDE)], wg),
        (wq_hbm, wq),
        (wk_hbm, wk),
        (wv_hbm, wv),
        (cum_hbm, cum),
        (keys_hbm, keys),
        (values_hbm, values),
        (wo_hbm, wo.at[tp]),
    )
    loads = [pltpu.make_async_copy(a, b, local_sems.at[i]) for i, (a, b) in enumerate(pairs)]
    for load in loads:
        load.start()

    loads[0].wait()

    @pl.when(owner)
    def _():
        lane = iota((PROPS, WIDE), 1)
        sub = iota((PROPS, WIDE), 0)
        parent = jnp.full((PROPS, WIDE), -1, jnp.int32)
        for j in range(PROPS):
            parent = jnp.where(sub == j, parents_ref[j, own_b], parent)
        seen = jnp.where((lane == sub) | (lane == parent), 1.0, 0.0)
        rest = jnp.zeros((WIDE - PROPS, WIDE), f32)
        for _ in range(4):
            square = jnp.concatenate([seen, rest], axis=0).astype(bf16)
            seen = jnp.minimum(dot_nn(seen.astype(bf16), square), 1.0)
        reach[...] = jnp.concatenate([seen, rest], axis=0)

    with jax.named_scope("wait_inputs"):
        for load in loads[4:10]:
            load.wait()
    x = tok[...].astype(f32)
    width = x.shape[0]
    eye = iota((width, width), 0) == iota((width, width), 1)
    gain_col = jnp.sum(jnp.where(eye, gain[...], 0.0), axis=1, keepdims=True)
    square_row = jnp.sum(x * x, axis=0, keepdims=True)
    scaled_t = x * gain_col
    scaled = jnp.transpose(scaled_t).astype(bf16)
    gate_w = wg[...].astype(f32)
    gate_w = jnp.where(lax.rem(me, 2) == 0, gate_w[:, :width], gate_w[:, width:]).astype(bf16)
    gates = dot_nn(gate_w, scaled_t.astype(bf16))
    gate_row = iota(gates.shape, 0)
    rows = [square_row] + [
        jnp.sum(jnp.where(gate_row == heads * tp + h, gates, 0.0), axis=0, keepdims=True)
        for h in range(heads)
    ]
    sub, lane = iota((8, WIDE), 0), iota((8, WIDE), 1)
    for j in range(3):
        tile = jnp.zeros((8, WIDE), f32)
        for k, row in enumerate(rows):
            part = row[:, j * WIDE : (j + 1) * WIDE]
            part = pltpu.roll(jnp.broadcast_to(part, (8, WIDE)), k * PROPS, 1)
            tile = jnp.where(sub == k, part, tile)
        for c in range(8):
            moved = pltpu.roll(tile, (WIDE - c * PROPS) % WIDE, 1)
            moved = jnp.where(lax.shift_right_logical(lane, 4) == sub, moved, 0.0)
            part_s[8 * j + c] = jnp.sum(moved, axis=0, keepdims=True)
    part_q[...] = dot_nn(scaled, wq[...]).astype(bf16).reshape(SEQS, PROPS, WIDE)
    part_n[:, :, :WIDE] = dot_nn(scaled, wk[...]).astype(bf16).reshape(SEQS, PROPS, WIDE)
    part_n[:, :, WIDE:] = dot_nn(scaled, wv[...]).astype(bf16).reshape(SEQS, PROPS, WIDE)

    with jax.named_scope("barrier"):
        pl.semaphore_wait(barrier, NKV - 1 + tp_count - 1)

    def remote(src, dst, send, recv, where):
        return pltpu.make_async_remote_copy(
            src_ref=src, dst_ref=dst, send_sem=send, recv_sem=recv, device_id=where
        )

    def to_owners(body):
        @pl.loop(0, NZ)
        def _(i):
            z = lax.rem(my_z + far_first(i), NZ)
            for r in range(3):
                peer = owner_of(z, r)

                @pl.when(peer != me)
                def _():
                    body(z + NZ * r, peer)

    def to_everyone(low, body):
        @pl.loop(0, NZ)
        def _(i):
            z = lax.rem(my_z + far_first(i), NZ)

            @pl.when(z >= low)
            def _():
                for k in range(NX):
                    body(z * NX + lax.rem(my_x + (2, 1, 3, 0)[k], NX))

    def to_all(low, body):
        def other(peer):
            @pl.when(peer != me)
            def _():
                body(peer)

        to_everyone(low, other)

    def send_queries(b, peer):
        remote(part_q.at[b], got_q.at[me], send_sems.at[0], recv_sems.at[0], {"kv": peer}).start()
        remote(part_s.at[b], got_s.at[me], send_sems.at[1], recv_sems.at[1], {"kv": peer}).start()

    def along_x(body):
        @pl.loop(0, NZ)
        def _(z):
            for r in range(3):
                body(z + NZ * r, z, lax.rem(z + 1 + r, NX))

    def in_column(body):
        @pl.loop(0, NZ)
        def _(i):
            z = lax.rem(my_z + far_first(i), NZ)
            r = lax.rem(my_x - z - 1 + 2 * NX * NZ, NX)

            @pl.when(r < 3)
            def _():
                body(lax.min(z + NZ * r, SEQS - 1), z)

    def send_new(b, z, x_at):
        slot = NX * z + my_x

        @pl.when(x_at != my_x)
        def _():
            there = {"kv": my_z * NX + x_at}
            remote(
                part_n.at[b], got_x.at[slot], send_sems.at[2], recv_sems.at[2], there
            ).start()

        @pl.when(x_at == my_x)
        def _():
            got_x[slot] = part_n[b]

    def pass_new(b, z):
        total = jnp.sum(got_x[pl.ds(NX * z, NX)].astype(f32), axis=0)
        sum_x[z] = total.astype(bf16)

    def send_sums(b, z):
        @pl.when(z != my_z)
        def _():
            there = {"kv": z * NX + my_x}
            remote(
                sum_x.at[z], got_n.at[my_z], send_sems.at[9], recv_sems.at[3], there
            ).start()

        @pl.when(z == my_z)
        def _():
            got_n[my_z] = sum_x[z]

    with jax.named_scope("send_parts"):
        to_owners(send_queries)

    loads[13].wait()

    @pl.loop(0, tp_count - 1)
    def _(i):
        there = {"tp": lax.rem(tp + i + 1, tp_count)}
        pl.semaphore_signal(planes_in, inc=1, device_id=there)
        remote(wo.at[tp], wo.at[tp], send_sems.at[8], recv_sems.at[5], there).start()

    along_x(send_new)

    with jax.named_scope("wait_cache"):
        for load in (loads[1], loads[2], loads[3], loads[10], loads[11]):
            load.wait()
    positions = offset + iota((1, length), 1)

    with jax.named_scope("prepare"):

        @pl.loop(0, SEQS)
        def _(b):
            filled = prior_ref[b] + accepted_ref[b]
            gates_b = cum[b]
            last = jnp.sum(
                jnp.where(positions == filled - 1, gates_b, 0.0), axis=1, keepdims=True
            )
            cum[b] = jnp.where(positions < filled, gates_b, MASKED)
            lane = iota((1, WIDE), 1)
            row = jnp.where(lane == 64, last[0:1], 0.0) + jnp.where(lane == 65, last[1:2], 0.0)
            out_s[b] = row
            keys_t[b] = jnp.transpose(keys[b])

    def arrived(ref, count, sem):
        some = ref.at[pl.ds(0, count)]
        pltpu.make_async_copy(some, some, sem).wait()

    sent = arrived

    def all_arrived(ref, sem):
        arrived(ref, NKV - 1, sem)

    def own_inverse(sums):
        return lax.rsqrt(as_column(sums, 0) / D + NORM_EPS)

    @pl.when(owner)
    def _():
        got_q[me] = part_q[own_b]
        got_s[me] = part_s[own_b]
        with jax.named_scope("wait_parts"):
            all_arrived(got_s, recv_sems.at[1])
            all_arrived(got_q, recv_sems.at[0])
        sums = jnp.sum(got_s[...], axis=0)
        inverse = own_inverse(sums)
        total = jnp.sum(got_q[...].astype(f32), axis=0)
        rounded = (inverse * total).astype(bf16).astype(f32)
        queries[own_b] = (rounded * HEAD**-0.5).astype(bf16)

        def send(peer):
            remote(
                queries.at[own_b],
                queries.at[own_b],
                send_sems.at[3],
                query_sems.at[my_z],
                {"kv": peer},
            ).start()

        with jax.named_scope("send_queries"):
            to_all(0, send)

    with jax.named_scope("pass_new"):
        arrived(got_x, SEQS - SEQS // NX, recv_sems.at[2])
        in_column(pass_new)
        in_column(send_sums)

    with jax.named_scope("wait_cache"):
        loads[12].wait()

    @pl.loop(0, NZ // 2)
    def _(i):
        pair = [lax.rem(my_z + near_first(2 * i + k), NZ) for k in range(2)]
        for z in pair:
            with jax.named_scope("wait_query"):
                mine_too = jnp.logical_and(owner, z == my_z)

                @pl.when(mine_too)
                def _():
                    arrived(queries, 2, query_sems.at[z])

                @pl.when(jnp.logical_not(mine_too))
                def _():
                    arrived(queries, 3, query_sems.at[z])

        group = [(z + NZ * r, owner_of(z, r)) for z in pair for r in range(3)]
        scores = []
        for b, _ in group:
            bias = cum[b]
            bias = jnp.concatenate(
                [jnp.broadcast_to(bias[h : h + 1], (PROPS, length)) for h in range(heads)], axis=0
            )
            query = split_heads(queries[b].astype(f32))
            scores.append(dot_nn(query, keys_t[b]) - bias)
        tops = [jnp.max(x, axis=1, keepdims=True) for x in scores]
        weights = [jnp.exp(x - top) for x, top in zip(scores, tops)]
        totals = [jnp.sum(x, axis=1, keepdims=True) for x in weights]
        blocks = [dot_nn(x.astype(bf16), values[b]) for x, (b, _) in zip(weights, group)]
        for k, (b, _) in enumerate(group):
            out_s[b] = out_s[b] + as_row(tops[k], totals[k])
            out_v[b] = join_heads(blocks[k]).astype(bf16)

        for b, peer in group:

            @pl.when(peer != me)
            def _():
                there = {"kv": peer}
                remote(
                    out_s.at[b], got_m.at[me], send_sems.at[4], recv_sems.at[7], there
                ).start()
                remote(
                    out_v.at[b], got_v.at[me], send_sems.at[5], recv_sems.at[4], there
                ).start()

    @pl.when(owner)
    def _():
        got_v[me] = out_v[own_b]
        got_m[me] = out_s[own_b]

        with jax.named_scope("wait_new"):
            arrived(got_n, NZ - 1, recv_sems.at[3])
        sums = jnp.sum(got_s[...], axis=0)
        inverse = own_inverse(sums)
        new = (inverse * jnp.sum(got_n[...].astype(f32), axis=0)).astype(bf16)
        own_new[...] = new

        for k in range(FIRST_WRITER, NZ):

            @pl.when(my_z != k)
            def _():
                there = {"kv": k * NX + my_x}
                remote(
                    own_new, new_ref.at[own_b], send_sems.at[6], recv_sems.at[6], there
                ).start()

        @pl.when(my_z >= FIRST_WRITER)
        def _():
            new_ref[own_b] = new

        seen = reach[...]
        seen_t = jnp.transpose(seen)[:PROPS]
        bias_rows = []
        for h in range(heads):
            logit = inverse * as_column(sums, PROPS * (h + 1)) + bias_ref[heads * tp + h]
            log_gate = jnp.minimum(logit, 0.0) - jnp.log1p(jnp.exp(-jnp.abs(logit)))
            tree_gate = jnp.sum(seen_t * log_gate, axis=0, keepdims=True)
            bias_rows.append(jnp.broadcast_to(tree_gate, (PROPS, WIDE)))
        rest = jnp.zeros((WIDE - PROPS, WIDE), bf16)
        new_keys = jnp.concatenate([new[:, :WIDE], rest], axis=0)
        new_values = jnp.concatenate([new[:, WIDE:], rest], axis=0)
        live = jnp.concatenate([seen[:PROPS], seen[:PROPS]], axis=0) > 0.5
        scores = dot_nt(split_heads(queries[own_b].astype(f32)), new_keys)
        scores = jnp.where(live, scores - jnp.concatenate(bias_rows, axis=0), -MASKED)
        top = jnp.max(scores, axis=1, keepdims=True)
        weights = jnp.where(live, jnp.exp(scores - top), 0.0)
        total = jnp.sum(weights, axis=1, keepdims=True)
        got_v[NKV] = join_heads(dot_nn(weights.astype(bf16), new_values)).astype(bf16)
        tree_row = as_row(top, total)

        with jax.named_scope("wait_stats"):
            all_arrived(got_m, recv_sems.at[7])
        lane = iota((1, WIDE), 1)
        stats = got_m[pl.ds(0, NKV)]
        ends = jnp.sum(stats, axis=0)
        last_0 = jnp.sum(jnp.where(lane == 64, ends, 0.0), axis=1, keepdims=True)
        last_1 = jnp.sum(jnp.where(lane == 65, ends, 0.0), axis=1, keepdims=True)
        shift = jnp.where(lane < PROPS, last_0, jnp.where(lane < 2 * PROPS, last_1, 0.0))
        got_m[NKV] = tree_row - shift
        stats = got_m[...]
        top = jnp.max(stats, axis=0, keepdims=True)
        held = lane.reshape(1, 1, WIDE) < 2 * PROPS
        factors = jnp.exp(jnp.where(held, stats - top, 0.0))
        sums_in = jnp.concatenate([stats[:, :, 32:], stats[:, :, :32]], axis=2)
        grand = jnp.sum(factors * sums_in, axis=0, keepdims=True)
        shares = factors / jnp.where(held, grand, 1.0)
        with jax.named_scope("wait_blocks"):
            all_arrived(got_v, recv_sems.at[4])
        first = iota((PROPS, WIDE), 1) < HEAD
        result = jnp.zeros((PROPS, WIDE), f32)
        for s in range(NKV + 1):
            share = shares[s]
            pair = jnp.where(first, as_column(share, 0), as_column(share, PROPS))
            result = result + pair * got_v[s].astype(f32)
        own_rows[...] = result.astype(bf16)
        slot = lax.rem(own_b, per)

        if tp_count > 1:
            pl.semaphore_wait(planes_in, tp_count - 1)

        def send_rows(peer):
            @pl.when(jnp.logical_or(peer != me, own_to != tp))
            def _():
                remote(
                    own_rows,
                    got_rows.at[tp, slot],
                    send_sems.at[7],
                    row_sems.at[tp],
                    {"kv": peer, "tp": own_to},
                ).start()

        with jax.named_scope("send_rows"):
            to_everyone(0, send_rows)

        @pl.when(own_to == tp)
        def _():
            got_rows[tp, slot] = own_rows[...]

    @pl.when(my_z >= FIRST_WRITER)
    def _():
        with jax.named_scope("wait_column"):

            @pl.when(owner)
            def _():
                arrived(new_ref, SEQS // NX - 1, recv_sems.at[6])

            @pl.when(jnp.logical_not(owner))
            def _():
                arrived(new_ref, SEQS // NX, recv_sems.at[6])

        def pass_on(b, z):
            for k in range(1, NX):
                there = {"kv": my_z * NX + lax.rem(my_x + k, NX)}
                remote(
                    new_ref.at[b], new_ref.at[b], send_sems.at[10], recv_sems.at[8], there
                ).start()

        in_column(pass_on)

    def sent_to_owners(count):
        sent(part_q, count, send_sems.at[0])
        sent(part_s, count, send_sems.at[1])
        sent(out_s, count, send_sems.at[4])
        sent(out_v, count, send_sems.at[5])
        sent(got_x, count - SEQS // NX * (NX - 1), send_sems.at[9])

    sent(got_x, SEQS - SEQS // NX, send_sems.at[2])

    @pl.when(owner)
    def _():
        sent_to_owners(SEQS - 1)
        sent(got_v, NKV - 1, send_sems.at[3])

        @pl.when(own_to == tp)
        def _():
            sent(got_v, NKV - 1, send_sems.at[7])

        @pl.when(own_to != tp)
        def _():
            sent(got_v, NKV, send_sems.at[7])

        @pl.when(my_z >= FIRST_WRITER)
        def _():
            sent(got_x, NZ - FIRST_WRITER - 1, send_sems.at[6])

        @pl.when(my_z < FIRST_WRITER)
        def _():
            sent(got_x, NZ - FIRST_WRITER, send_sems.at[6])

    @pl.when(jnp.logical_not(owner))
    def _():
        sent_to_owners(SEQS)

    if tp_count > 1:

        @pl.when(jnp.logical_not(owner))
        def _():
            pl.semaphore_wait(planes_in, tp_count - 1)

        sent(wo, tp_count - 1, send_sems.at[8])

    @pl.when(my_z >= FIRST_WRITER)
    def _():
        sent(got_x, SEQS - SEQS // NX, send_sems.at[10])

        with jax.named_scope("wait_fresh"):
            arrived(new_ref, SEQS - SEQS // NX, recv_sems.at[8])

    if tp_count > 1:
        arrived(wo, tp_count - 1, recv_sems.at[5])

    total = jnp.zeros((per * PROPS, wo.shape[1]), f32)
    for k in range(tp_count):
        plane = lax.rem(tp + k, tp_count)
        with jax.named_scope("wait_rows"):
            if k == 0:
                mine_too = jnp.logical_and(owner, own_to == tp)

                @pl.when(mine_too)
                def _():
                    arrived(got_v, per - 1, row_sems.at[plane])

                @pl.when(jnp.logical_not(mine_too))
                def _():
                    arrived(got_v, per, row_sems.at[plane])

            else:
                arrived(got_v, per, row_sems.at[plane])
        with jax.named_scope("project"):
            rows_in = got_rows[plane].reshape(per * PROPS, WIDE)
            total = total + dot_nt(rows_in, wo[plane])
    mixed_ref[...] = total.astype(bf16)


def write_kernel(
    mixed_in, new_ref, prior_ref, accepted_ref, keys, values,
    mixed_out, keys_out, values_out, sems_out, sem_mixed,
):
    me = lax.axis_index("kv")
    length = keys.shape[1]
    both = ((keys, keys_out), (values, values_out))

    def copy_out(k, b):
        return pltpu.make_async_copy(both[k][0].at[b], both[k][1].at[b], sems_out.at[k])

    mixed = pltpu.make_async_copy(mixed_in, mixed_out, sem_mixed)
    mixed.start()

    @pl.loop(0, SEQS)
    def _(b):
        start = prior_ref[b] + accepted_ref[b] - me * length

        @pl.when((start > -PROPS) & (start < length))
        def _():
            base = jnp.clip(lax.shift_right_arithmetic(start, 4), 0, length // PROPS - 2) * PROPS
            rows = pl.ds(pl.multiple_of(base, PROPS), 2 * PROPS)
            slot = iota((2 * PROPS, PROPS), 0) + (base - start)
            pick = jnp.where(slot == iota((2 * PROPS, PROPS), 1), 1.0, 0.0).astype(bf16)
            placed = dot_nn(pick, new_ref[b])
            at = iota((2 * PROPS, WIDE), 0) + (base - start)
            inside = (at >= 0) & (at < PROPS)
            for k in range(2):
                held = both[k][0]
                old = held[b, rows, :].astype(f32)
                fresh = placed[:, k * WIDE : (k + 1) * WIDE]
                held[b, rows, :] = jnp.where(inside, fresh, old).astype(bf16)

        for k in range(2):
            copy_out(k, b).start()

    with jax.named_scope("write_wait"):

        for k in range(2):
            pltpu.make_async_copy(both[k][0], both[k][1], sems_out.at[k]).wait()

    mixed.wait()


def on_chip(shape, dtype):
    return pltpu.VMEM(shape, dtype)


def shards(
    tokens, norm_gain, w_query, w_key, w_value, w_gate, gate_bias, w_out,
    keys_cache, values_cache, cum_gates, prior_len, accepted, parents,
):
    tp_count = lax.axis_size("tp")
    rows, width = tokens.shape
    columns = w_out.shape[1]
    length = keys_cache.shape[1]
    any_ = pl.BlockSpec(memory_space=pl.ANY)
    smem = pl.BlockSpec(memory_space=pltpu.SMEM)
    vmem = pl.BlockSpec(memory_space=pltpu.VMEM)
    out_rows = rows // tp_count
    dma = pltpu.SemaphoreType.DMA
    mixed, new, keys_held, values_held = pl.pallas_call(
        functools.partial(step_kernel, tp_count),
        out_shape=(
            on_chip((out_rows, columns), bf16),
            on_chip((SEQS, PROPS, 2 * WIDE), bf16),
            on_chip(keys_cache.shape, bf16),
            on_chip(values_cache.shape, bf16),
        ),
        in_specs=[pl.BlockSpec(memory_space=pltpu.HBM)] * 14,
        out_specs=(vmem, vmem, vmem, vmem),
        scratch_shapes=[
            pltpu.SMEM(gate_bias.shape, f32),
            pltpu.SMEM(prior_len.shape, jnp.int32),
            pltpu.SMEM(accepted.shape, jnp.int32),
            pltpu.SMEM(parents.shape[::-1], jnp.int32),
            pltpu.VMEM((width, rows), bf16),
            pltpu.VMEM((1, width), f32),
            pltpu.VMEM((width, WIDE), bf16),
            pltpu.VMEM((width, WIDE), bf16),
            pltpu.VMEM((width, WIDE), bf16),
            pltpu.VMEM((w_gate.shape[1], WIDE), bf16),
            pltpu.VMEM((tp_count, columns, WIDE), bf16),
            pltpu.VMEM((SEQS, WIDE, length), bf16),
            pltpu.VMEM(cum_gates.shape, f32),
            pltpu.VMEM((SEQS, PROPS, WIDE), bf16),
            pltpu.VMEM((SEQS, PROPS, 2 * WIDE), bf16),
            pltpu.VMEM((SEQS, 1, WIDE), f32),
            pltpu.VMEM((NKV, PROPS, WIDE), bf16),
            pltpu.VMEM((NZ * NX, PROPS, 2 * WIDE), bf16),
            pltpu.VMEM((NZ, PROPS, 2 * WIDE), bf16),
            pltpu.VMEM((NZ, PROPS, 2 * WIDE), bf16),
            pltpu.VMEM((NKV, 1, WIDE), f32),
            pltpu.VMEM((SEQS, PROPS, WIDE), bf16),
            pltpu.VMEM((PROPS, 2 * WIDE), bf16),
            pltpu.VMEM((SEQS, PROPS, WIDE), bf16),
            pltpu.VMEM((SEQS, 1, WIDE), f32),
            pltpu.VMEM((NKV + 1, PROPS, WIDE), bf16),
            pltpu.VMEM((NKV + 1, 1, WIDE), f32),
            pltpu.VMEM((PROPS, WIDE), bf16),
            pltpu.VMEM((tp_count, SEQS // tp_count, PROPS, WIDE), bf16),
            pltpu.VMEM((WIDE, WIDE), f32),
            dma((14,)),
            dma((11,)),
            dma((9,)),
            dma((NZ,)),
            dma((tp_count,)),
            pltpu.SemaphoreType.REGULAR,
        ],
        compiler_params=pltpu.CompilerParams(
            collective_id=0, has_side_effects=True, vmem_limit_bytes=24 << 20
        ),
        name="tree_step",
    )(
        *(
            pltpu.with_memory_space_constraint(x, pltpu.HBM)
            for x in (
                tokens.T, norm_gain.reshape(1, width), w_query, w_key, w_value, w_gate.T, w_out.T,
                keys_cache, values_cache, cum_gates, gate_bias, prior_len, accepted, parents.T,
            )
        )
    )

    def held(x):
        return pltpu.with_memory_space_constraint(x, pltpu.VMEM)

    return pl.pallas_call(
        write_kernel,
        out_shape=(
            jax.ShapeDtypeStruct((out_rows, columns), bf16),
            jax.ShapeDtypeStruct(keys_cache.shape, bf16),
            jax.ShapeDtypeStruct(values_cache.shape, bf16),
        ),
        in_specs=[vmem, vmem, smem, smem, vmem, vmem],
        out_specs=(any_, any_, any_),
        scratch_shapes=[dma((2,)), dma],
        compiler_params=pltpu.CompilerParams(vmem_limit_bytes=8 << 20),
        name="cache_write",
    )(held(mixed), held(new), prior_len, accepted, held(keys_held), held(values_held))


def solution(mesh):
    in_specs = (
        P(None, "kv"),
        P("kv"),
        P("kv", "tp"),
        P("kv", "tp"),
        P("kv", "tp"),
        P(),
        P(),
        P("tp", "kv"),
        P(None, "kv", "tp"),
        P(None, "kv", "tp"),
        P(None, "tp", "kv"),
        P(),
        P(),
        P(),
    )
    out_specs = (P("tp", "kv"), P(None, "kv", "tp"), P(None, "kv", "tp"))
    return jax.shard_map(
        shards, mesh=mesh, in_specs=in_specs, out_specs=out_specs, check_vma=False
    )
```

```python
import functools

import jax
import jax.numpy as jnp
from jax import lax
from jax.experimental import pallas as pl
from jax.experimental.pallas import tpu as pltpu
from jax.sharding import PartitionSpec as P

D = 2048
HEAD = 64
PROPS = 16
SEQS = 24
NZ, NX = 8, 4
NKV = NZ * NX
WIDE = 128
MASKED = 1e30
NORM_EPS = 1e-06
FIRST_WRITER = 4

f32, bf16 = jnp.float32, jnp.bfloat16


def iota(shape, dim):
    return lax.broadcasted_iota(jnp.int32, shape, dim)


def dot_nt(a, b):
    return lax.dot_general(a, b, (((1,), (1,)), ((), ())), preferred_element_type=f32)


def dot_nn(a, b):
    return lax.dot_general(a, b, (((1,), (0,)), ((), ())), preferred_element_type=f32)


def far_first(i):
    return 4 + (1 - 2 * lax.rem(i, 2)) * lax.div(i + 1, 2)


def near_first(i):
    odd = lax.rem(i, 2)
    return odd * lax.div(i + 1, 2) + (1 - odd) * lax.rem(NZ - lax.div(i, 2), NZ)


def owner_of(z, r):
    return z * NX + lax.rem(z + 1 + r, NX)


def split_heads(rows):
    lane = iota((2 * PROPS, WIDE), 1)
    sub = iota((2 * PROPS, WIDE), 0)
    both = jnp.concatenate([rows, rows], axis=0)
    return jnp.where((lane < HEAD) == (sub < PROPS), both, 0.0).astype(bf16)


def join_heads(rows):
    lane = iota((PROPS, WIDE), 1)
    return jnp.where(lane < HEAD, rows[:PROPS], rows[PROPS:])


def as_row(tops, sums):
    lane = iota((2 * PROPS, WIDE), 1)
    sub = iota((2 * PROPS, WIDE), 0)
    spread = jnp.where(lane == sub, tops, jnp.where(lane == sub + 2 * PROPS, sums, 0.0))
    return jnp.sum(spread, axis=0, keepdims=True)


def as_column(row, start):
    lane = iota((PROPS, WIDE), 1)
    sub = iota((PROPS, WIDE), 0)
    return jnp.sum(jnp.where(lane == sub + start, row, 0.0), axis=1, keepdims=True)


def step_kernel(
    tp_count,
    tok_hbm,
    gain_hbm,
    wq_hbm,
    wk_hbm,
    wv_hbm,
    wg_hbm,
    wo_hbm,
    keys_hbm,
    values_hbm,
    cum_hbm,
    bias_hbm,
    prior_hbm,
    accepted_hbm,
    parents_hbm,
    mixed_ref,
    new_ref,
    keys,
    values,
    filled_ref,
    bias_ref,
    prior_ref,
    accepted_ref,
    parents_ref,
    tok,
    gain,
    wq,
    wk,
    wv,
    wg,
    wo,
    keys_t,
    cum,
    part_q,
    part_n,
    part_s,
    got_q,
    got_x,
    sum_x,
    got_n,
    got_s,
    queries,
    own_new,
    out_v,
    out_s,
    got_v,
    got_m,
    own_rows,
    got_rows,
    reach,
    local_sems,
    send_sems,
    recv_sems,
    query_sems,
    row_sems,
    planes_in,
):
    me = lax.axis_index("kv")
    tp = lax.axis_index("tp")
    my_z, my_x = lax.div(me, NX), lax.rem(me, NX)
    my_r = lax.rem(my_x - my_z - 1 + 2 * NX * NZ, NX)
    owner = my_r < 3
    own_b = lax.min(my_z + NZ * my_r, SEQS - 1)
    per = SEQS // tp_count
    own_to = lax.div(own_b, per)
    length = keys.shape[1]
    offset = me * length
    heads = 2

    barrier = pltpu.get_barrier_semaphore()

    @pl.loop(0, NZ)
    def _(i):
        z = lax.rem(my_z + far_first(i), NZ)
        for k in range(NX):
            peer = z * NX + lax.rem(my_x + (2, 1, 3, 0)[k], NX)

            @pl.when(peer != me)
            def _():
                pl.semaphore_signal(barrier, inc=1, device_id={"kv": peer})

    @pl.loop(0, tp_count - 1)
    def _(i):
        pl.semaphore_signal(barrier, inc=1, device_id={"tp": lax.rem(tp + i + 1, tp_count)})

    gate_block = pl.multiple_of(lax.div(me, 2) * WIDE, WIDE)
    pairs = (
        (parents_hbm, parents_ref),
        (bias_hbm, bias_ref),
        (prior_hbm, prior_ref),
        (accepted_hbm, accepted_ref),
        (tok_hbm, tok),
        (gain_hbm, gain),
        (wg_hbm.at[:, pl.ds(gate_block, WIDE)], wg),
        (wq_hbm, wq),
        (wk_hbm, wk),
        (wv_hbm, wv),
        (cum_hbm, cum),
        (keys_hbm, keys),
        (values_hbm, values),
        (wo_hbm, wo.at[tp]),
    )
    loads = [pltpu.make_async_copy(a, b, local_sems.at[i]) for i, (a, b) in enumerate(pairs)]
    for load in loads:
        load.start()

    loads[0].wait()

    @pl.when(owner)
    def _():
        lane = iota((PROPS, WIDE), 1)
        sub = iota((PROPS, WIDE), 0)
        parent = jnp.full((PROPS, WIDE), -1, jnp.int32)
        for j in range(PROPS):
            parent = jnp.where(sub == j, parents_ref[j, own_b], parent)
        seen = jnp.where((lane == sub) | (lane == parent), 1.0, 0.0)
        rest = jnp.zeros((WIDE - PROPS, WIDE), f32)
        for _ in range(4):
            square = jnp.concatenate([seen, rest], axis=0).astype(bf16)
            seen = jnp.minimum(dot_nn(seen.astype(bf16), square), 1.0)
        reach[...] = jnp.concatenate([seen, rest], axis=0)

    with jax.named_scope("wait_inputs"):
        for load in loads[4:10]:
            load.wait()
    x = tok[...].astype(f32)
    width = x.shape[0]
    eye = iota((width, width), 0) == iota((width, width), 1)
    gain_col = jnp.sum(jnp.where(eye, gain[...], 0.0), axis=1, keepdims=True)
    square_row = jnp.sum(x * x, axis=0, keepdims=True)
    scaled_t = x * gain_col
    scaled = jnp.transpose(scaled_t).astype(bf16)
    gate_w = wg[...].astype(f32)
    gate_w = jnp.where(lax.rem(me, 2) == 0, gate_w[:, :width], gate_w[:, width:]).astype(bf16)
    gates = dot_nn(gate_w, scaled_t.astype(bf16))
    gate_row = iota(gates.shape, 0)
    rows = [square_row] + [
        jnp.sum(jnp.where(gate_row == heads * tp + h, gates, 0.0), axis=0, keepdims=True)
        for h in range(heads)
    ]
    sub, lane = iota((8, WIDE), 0), iota((8, WIDE), 1)
    for j in range(3):
        tile = jnp.zeros((8, WIDE), f32)
        for k, row in enumerate(rows):
            part = row[:, j * WIDE : (j + 1) * WIDE]
            part = pltpu.roll(jnp.broadcast_to(part, (8, WIDE)), k * PROPS, 1)
            tile = jnp.where(sub == k, part, tile)
        for c in range(8):
            moved = pltpu.roll(tile, (WIDE - c * PROPS) % WIDE, 1)
            moved = jnp.where(lax.shift_right_logical(lane, 4) == sub, moved, 0.0)
            part_s[8 * j + c] = jnp.sum(moved, axis=0, keepdims=True)
    part_q[...] = dot_nn(scaled, wq[...]).astype(bf16).reshape(SEQS, PROPS, WIDE)
    part_n[:, :, :WIDE] = dot_nn(scaled, wk[...]).astype(bf16).reshape(SEQS, PROPS, WIDE)
    part_n[:, :, WIDE:] = dot_nn(scaled, wv[...]).astype(bf16).reshape(SEQS, PROPS, WIDE)

    with jax.named_scope("barrier"):
        pl.semaphore_wait(barrier, NKV - 1 + tp_count - 1)

    def remote(src, dst, send, recv, where):
        return pltpu.make_async_remote_copy(
            src_ref=src, dst_ref=dst, send_sem=send, recv_sem=recv, device_id=where
        )

    def to_owners(body):
        @pl.loop(0, NZ)
        def _(i):
            z = lax.rem(my_z + far_first(i), NZ)
            for r in range(3):
                peer = owner_of(z, r)

                @pl.when(peer != me)
                def _():
                    body(z + NZ * r, peer)

    def to_everyone(low, body):
        @pl.loop(0, NZ)
        def _(i):
            z = lax.rem(my_z + far_first(i), NZ)

            @pl.when(z >= low)
            def _():
                for k in range(NX):
                    body(z * NX + lax.rem(my_x + (2, 1, 3, 0)[k], NX))

    def to_all(low, body):
        def other(peer):
            @pl.when(peer != me)
            def _():
                body(peer)

        to_everyone(low, other)

    def send_queries(b, peer):
        remote(part_q.at[b], got_q.at[me], send_sems.at[0], recv_sems.at[0], {"kv": peer}).start()
        remote(part_s.at[b], got_s.at[me], send_sems.at[1], recv_sems.at[1], {"kv": peer}).start()

    def along_x(body):
        @pl.loop(0, NZ)
        def _(z):
            for r in range(3):
                body(z + NZ * r, z, lax.rem(z + 1 + r, NX))

    def in_column(body):
        @pl.loop(0, NZ)
        def _(i):
            z = lax.rem(my_z + far_first(i), NZ)
            r = lax.rem(my_x - z - 1 + 2 * NX * NZ, NX)

            @pl.when(r < 3)
            def _():
                body(lax.min(z + NZ * r, SEQS - 1), z)

    def send_new(b, z, x_at):
        slot = NX * z + my_x

        @pl.when(x_at != my_x)
        def _():
            there = {"kv": my_z * NX + x_at}
            remote(
                part_n.at[b], got_x.at[slot], send_sems.at[2], recv_sems.at[2], there
            ).start()

        @pl.when(x_at == my_x)
        def _():
            got_x[slot] = part_n[b]

    def pass_new(b, z):
        total = jnp.sum(got_x[pl.ds(NX * z, NX)].astype(f32), axis=0)
        sum_x[z] = total.astype(bf16)

    def send_sums(b, z):
        @pl.when(z != my_z)
        def _():
            there = {"kv": z * NX + my_x}
            remote(
                sum_x.at[z], got_n.at[my_z], send_sems.at[9], recv_sems.at[3], there
            ).start()

        @pl.when(z == my_z)
        def _():
            got_n[my_z] = sum_x[z]

    with jax.named_scope("send_parts"):
        to_owners(send_queries)

    loads[13].wait()

    @pl.loop(0, tp_count - 1)
    def _(i):
        there = {"tp": lax.rem(tp + i + 1, tp_count)}
        pl.semaphore_signal(planes_in, inc=1, device_id=there)
        remote(wo.at[tp], wo.at[tp], send_sems.at[8], recv_sems.at[5], there).start()

    along_x(send_new)

    with jax.named_scope("wait_cache"):
        for load in (loads[1], loads[2], loads[3], loads[10], loads[11]):
            load.wait()
    positions = offset + iota((1, length), 1)

    for b in range(SEQS):
        filled_ref[b] = prior_ref[b] + accepted_ref[b]

    with jax.named_scope("prepare"):

        @pl.loop(0, SEQS)
        def _(b):
            filled = prior_ref[b] + accepted_ref[b]
            gates_b = cum[b]
            last = jnp.sum(
                jnp.where(positions == filled - 1, gates_b, 0.0), axis=1, keepdims=True
            )
            cum[b] = jnp.where(positions < filled, gates_b, MASKED)
            lane = iota((1, WIDE), 1)
            row = jnp.where(lane == 64, last[0:1], 0.0) + jnp.where(lane == 65, last[1:2], 0.0)
            out_s[b] = row
            keys_t[b] = jnp.transpose(keys[b])

    def arrived(ref, count, sem):
        some = ref.at[pl.ds(0, count)]
        pltpu.make_async_copy(some, some, sem).wait()

    sent = arrived

    def all_arrived(ref, sem):
        arrived(ref, NKV - 1, sem)

    def own_inverse(sums):
        return lax.rsqrt(as_column(sums, 0) / D + NORM_EPS)

    @pl.when(owner)
    def _():
        got_q[me] = part_q[own_b]
        got_s[me] = part_s[own_b]
        with jax.named_scope("wait_parts"):
            all_arrived(got_s, recv_sems.at[1])
            all_arrived(got_q, recv_sems.at[0])
        sums = jnp.sum(got_s[...], axis=0)
        inverse = own_inverse(sums)
        total = jnp.sum(got_q[...].astype(f32), axis=0)
        rounded = (inverse * total).astype(bf16).astype(f32)
        queries[own_b] = (rounded * HEAD**-0.5).astype(bf16)

        def send(peer):
            remote(
                queries.at[own_b],
                queries.at[own_b],
                send_sems.at[3],
                query_sems.at[my_z],
                {"kv": peer},
            ).start()

        with jax.named_scope("send_queries"):
            to_all(0, send)

    with jax.named_scope("pass_new"):
        arrived(got_x, SEQS - SEQS // NX, recv_sems.at[2])
        in_column(pass_new)
        in_column(send_sums)

    with jax.named_scope("wait_cache"):
        loads[12].wait()

    @pl.loop(0, NZ // 4)
    def _(i):
        pair = [lax.rem(my_z + far_first(4 * i + k), NZ) for k in range(4)]
        for z in pair:
            with jax.named_scope("wait_query"):
                mine_too = jnp.logical_and(owner, z == my_z)

                @pl.when(mine_too)
                def _():
                    arrived(queries, 2, query_sems.at[z])

                @pl.when(jnp.logical_not(mine_too))
                def _():
                    arrived(queries, 3, query_sems.at[z])

        group = [(z + NZ * r, owner_of(z, r)) for z in pair for r in range(3)]
        scores = []
        for b, _ in group:
            bias = cum[b]
            bias = jnp.concatenate(
                [jnp.broadcast_to(bias[h : h + 1], (PROPS, length)) for h in range(heads)], axis=0
            )
            query = split_heads(queries[b].astype(f32))
            scores.append(dot_nn(query, keys_t[b]) - bias)
        tops = [jnp.max(x, axis=1, keepdims=True) for x in scores]
        weights = [jnp.exp(x - top) for x, top in zip(scores, tops)]
        totals = [jnp.sum(x, axis=1, keepdims=True) for x in weights]
        blocks = [dot_nn(x.astype(bf16), values[b]) for x, (b, _) in zip(weights, group)]
        for k, (b, _) in enumerate(group):
            out_s[b] = out_s[b] + as_row(tops[k], totals[k])
            out_v[b] = join_heads(blocks[k]).astype(bf16)

        for b, peer in group:

            @pl.when(peer != me)
            def _():
                there = {"kv": peer}
                remote(
                    out_s.at[b], got_m.at[me], send_sems.at[4], recv_sems.at[7], there
                ).start()
                remote(
                    out_v.at[b], got_v.at[me], send_sems.at[5], recv_sems.at[4], there
                ).start()

    @pl.when(owner)
    def _():
        got_v[me] = out_v[own_b]
        got_m[me] = out_s[own_b]

        with jax.named_scope("wait_new"):
            arrived(got_n, NZ - 1, recv_sems.at[3])
        sums = jnp.sum(got_s[...], axis=0)
        inverse = own_inverse(sums)
        new = (inverse * jnp.sum(got_n[...].astype(f32), axis=0)).astype(bf16)
        own_new[...] = new

        for k in range(FIRST_WRITER, NZ):

            @pl.when(my_z != k)
            def _():
                there = {"kv": k * NX + my_x}
                remote(
                    own_new, new_ref.at[own_b], send_sems.at[6], recv_sems.at[6], there
                ).start()

        @pl.when(my_z >= FIRST_WRITER)
        def _():
            new_ref[own_b] = new

        seen = reach[...]
        seen_t = jnp.transpose(seen)[:PROPS]
        bias_rows = []
        for h in range(heads):
            logit = inverse * as_column(sums, PROPS * (h + 1)) + bias_ref[heads * tp + h]
            log_gate = jnp.minimum(logit, 0.0) - jnp.log1p(jnp.exp(-jnp.abs(logit)))
            tree_gate = jnp.sum(seen_t * log_gate, axis=0, keepdims=True)
            bias_rows.append(jnp.broadcast_to(tree_gate, (PROPS, WIDE)))
        rest = jnp.zeros((WIDE - PROPS, WIDE), bf16)
        new_keys = jnp.concatenate([new[:, :WIDE], rest], axis=0)
        new_values = jnp.concatenate([new[:, WIDE:], rest], axis=0)
        live = jnp.concatenate([seen[:PROPS], seen[:PROPS]], axis=0) > 0.5
        scores = dot_nt(split_heads(queries[own_b].astype(f32)), new_keys)
        scores = jnp.where(live, scores - jnp.concatenate(bias_rows, axis=0), -MASKED)
        top = jnp.max(scores, axis=1, keepdims=True)
        weights = jnp.where(live, jnp.exp(scores - top), 0.0)
        total = jnp.sum(weights, axis=1, keepdims=True)
        got_v[NKV] = join_heads(dot_nn(weights.astype(bf16), new_values)).astype(bf16)
        tree_row = as_row(top, total)

        with jax.named_scope("wait_stats"):
            all_arrived(got_m, recv_sems.at[7])
        lane = iota((1, WIDE), 1)
        stats = got_m[pl.ds(0, NKV)]
        ends = jnp.sum(stats, axis=0)
        last_0 = jnp.sum(jnp.where(lane == 64, ends, 0.0), axis=1, keepdims=True)
        last_1 = jnp.sum(jnp.where(lane == 65, ends, 0.0), axis=1, keepdims=True)
        shift = jnp.where(lane < PROPS, last_0, jnp.where(lane < 2 * PROPS, last_1, 0.0))
        got_m[NKV] = tree_row - shift
        stats = got_m[...]
        top = jnp.max(stats, axis=0, keepdims=True)
        held = lane.reshape(1, 1, WIDE) < 2 * PROPS
        factors = jnp.exp(jnp.where(held, stats - top, 0.0))
        sums_in = jnp.concatenate([stats[:, :, 32:], stats[:, :, :32]], axis=2)
        grand = jnp.sum(factors * sums_in, axis=0, keepdims=True)
        shares = factors / jnp.where(held, grand, 1.0)
        with jax.named_scope("wait_blocks"):
            all_arrived(got_v, recv_sems.at[4])
        first = iota((PROPS, WIDE), 1) < HEAD
        result = jnp.zeros((PROPS, WIDE), f32)
        for s in range(NKV + 1):
            share = shares[s]
            pair = jnp.where(first, as_column(share, 0), as_column(share, PROPS))
            result = result + pair * got_v[s].astype(f32)
        own_rows[...] = result.astype(bf16)
        slot = lax.rem(own_b, per)

        if tp_count > 1:
            pl.semaphore_wait(planes_in, tp_count - 1)

        def send_rows(peer):
            @pl.when(jnp.logical_or(peer != me, own_to != tp))
            def _():
                remote(
                    own_rows,
                    got_rows.at[tp, slot],
                    send_sems.at[7],
                    row_sems.at[tp],
                    {"kv": peer, "tp": own_to},
                ).start()

        with jax.named_scope("send_rows"):
            to_everyone(0, send_rows)

        @pl.when(own_to == tp)
        def _():
            got_rows[tp, slot] = own_rows[...]

    @pl.when(my_z >= FIRST_WRITER)
    def _():
        with jax.named_scope("wait_column"):

            @pl.when(owner)
            def _():
                arrived(new_ref, SEQS // NX - 1, recv_sems.at[6])

            @pl.when(jnp.logical_not(owner))
            def _():
                arrived(new_ref, SEQS // NX, recv_sems.at[6])

        def pass_on(b, z):
            for k in range(1, NX):
                there = {"kv": my_z * NX + lax.rem(my_x + k, NX)}
                remote(
                    new_ref.at[b], new_ref.at[b], send_sems.at[10], recv_sems.at[8], there
                ).start()

        in_column(pass_on)

    def sent_to_owners(count):
        sent(part_q, count, send_sems.at[0])
        sent(part_s, count, send_sems.at[1])
        sent(out_s, count, send_sems.at[4])
        sent(out_v, count, send_sems.at[5])
        sent(got_x, count - SEQS // NX * (NX - 1), send_sems.at[9])

    sent(got_x, SEQS - SEQS // NX, send_sems.at[2])

    @pl.when(owner)
    def _():
        sent_to_owners(SEQS - 1)
        sent(got_v, NKV - 1, send_sems.at[3])

        @pl.when(own_to == tp)
        def _():
            sent(got_v, NKV - 1, send_sems.at[7])

        @pl.when(own_to != tp)
        def _():
            sent(got_v, NKV, send_sems.at[7])

        @pl.when(my_z >= FIRST_WRITER)
        def _():
            sent(got_x, NZ - FIRST_WRITER - 1, send_sems.at[6])

        @pl.when(my_z < FIRST_WRITER)
        def _():
            sent(got_x, NZ - FIRST_WRITER, send_sems.at[6])

    @pl.when(jnp.logical_not(owner))
    def _():
        sent_to_owners(SEQS)

    if tp_count > 1:

        @pl.when(jnp.logical_not(owner))
        def _():
            pl.semaphore_wait(planes_in, tp_count - 1)

        sent(wo, tp_count - 1, send_sems.at[8])

    @pl.when(my_z >= FIRST_WRITER)
    def _():
        sent(got_x, SEQS - SEQS // NX, send_sems.at[10])

        with jax.named_scope("wait_fresh"):
            arrived(new_ref, SEQS - SEQS // NX, recv_sems.at[8])

    if tp_count > 1:
        arrived(wo, tp_count - 1, recv_sems.at[5])

    total = jnp.zeros((per * PROPS, wo.shape[1]), f32)
    for k in range(tp_count):
        plane = lax.rem(tp + k, tp_count)
        with jax.named_scope("wait_rows"):
            if k == 0:
                mine_too = jnp.logical_and(owner, own_to == tp)

                @pl.when(mine_too)
                def _():
                    arrived(got_v, per - 1, row_sems.at[plane])

                @pl.when(jnp.logical_not(mine_too))
                def _():
                    arrived(got_v, per, row_sems.at[plane])

            else:
                arrived(got_v, per, row_sems.at[plane])
        with jax.named_scope("project"):
            rows_in = got_rows[plane].reshape(per * PROPS, WIDE)
            total = total + dot_nt(rows_in, wo[plane])
    mixed_ref[...] = total.astype(bf16)


def write_kernel(
    mixed_in, new_ref, filled_ref, keys, values,
    mixed_out, keys_out, values_out, sems_out, sem_mixed,
):
    me = lax.axis_index("kv")
    length = keys.shape[1]
    both = ((keys, keys_out), (values, values_out))

    def copy_out(k, b):
        return pltpu.make_async_copy(both[k][0].at[b], both[k][1].at[b], sems_out.at[k])

    mixed = pltpu.make_async_copy(mixed_in, mixed_out, sem_mixed)
    mixed.start()

    @pl.loop(0, SEQS)
    def _(b):
        start = filled_ref[b] - me * length

        @pl.when((start > -PROPS) & (start < length))
        def _():
            base = jnp.clip(lax.shift_right_arithmetic(start, 4), 0, length // PROPS - 2) * PROPS
            rows = pl.ds(pl.multiple_of(base, PROPS), 2 * PROPS)
            slot = iota((2 * PROPS, PROPS), 0) + (base - start)
            pick = jnp.where(slot == iota((2 * PROPS, PROPS), 1), 1.0, 0.0).astype(bf16)
            placed = dot_nn(pick, new_ref[b])
            at = iota((2 * PROPS, WIDE), 0) + (base - start)
            inside = (at >= 0) & (at < PROPS)
            for k in range(2):
                held = both[k][0]
                old = held[b, rows, :].astype(f32)
                fresh = placed[:, k * WIDE : (k + 1) * WIDE]
                held[b, rows, :] = jnp.where(inside, fresh, old).astype(bf16)

        for k in range(2):
            copy_out(k, b).start()

    with jax.named_scope("write_wait"):

        for k in range(2):
            pltpu.make_async_copy(both[k][0], both[k][1], sems_out.at[k]).wait()

    mixed.wait()


def on_chip(shape, dtype):
    return pltpu.VMEM(shape, dtype)


def scalars(shape, dtype):
    return pltpu.SMEM(shape, dtype)


def shards(
    tokens, norm_gain, w_query, w_key, w_value, w_gate, gate_bias, w_out,
    keys_cache, values_cache, cum_gates, prior_len, accepted, parents,
):
    tp_count = lax.axis_size("tp")
    rows, width = tokens.shape
    columns = w_out.shape[1]
    length = keys_cache.shape[1]
    any_ = pl.BlockSpec(memory_space=pl.ANY)
    smem = pl.BlockSpec(memory_space=pltpu.SMEM)
    vmem = pl.BlockSpec(memory_space=pltpu.VMEM)
    out_rows = rows // tp_count
    dma = pltpu.SemaphoreType.DMA
    mixed, new, keys_held, values_held, filled = pl.pallas_call(
        functools.partial(step_kernel, tp_count),
        out_shape=(
            on_chip((out_rows, columns), bf16),
            on_chip((SEQS, PROPS, 2 * WIDE), bf16),
            on_chip(keys_cache.shape, bf16),
            on_chip(values_cache.shape, bf16),
            scalars(prior_len.shape, jnp.int32),
        ),
        in_specs=[pl.BlockSpec(memory_space=pltpu.HBM)] * 14,
        out_specs=(vmem, vmem, vmem, vmem, smem),
        scratch_shapes=[
            pltpu.SMEM(gate_bias.shape, f32),
            pltpu.SMEM(prior_len.shape, jnp.int32),
            pltpu.SMEM(accepted.shape, jnp.int32),
            pltpu.SMEM(parents.shape[::-1], jnp.int32),
            pltpu.VMEM((width, rows), bf16),
            pltpu.VMEM((1, width), f32),
            pltpu.VMEM((width, WIDE), bf16),
            pltpu.VMEM((width, WIDE), bf16),
            pltpu.VMEM((width, WIDE), bf16),
            pltpu.VMEM((w_gate.shape[1], WIDE), bf16),
            pltpu.VMEM((tp_count, columns, WIDE), bf16),
            pltpu.VMEM((SEQS, WIDE, length), bf16),
            pltpu.VMEM(cum_gates.shape, f32),
            pltpu.VMEM((SEQS, PROPS, WIDE), bf16),
            pltpu.VMEM((SEQS, PROPS, 2 * WIDE), bf16),
            pltpu.VMEM((SEQS, 1, WIDE), f32),
            pltpu.VMEM((NKV, PROPS, WIDE), bf16),
            pltpu.VMEM((NZ * NX, PROPS, 2 * WIDE), bf16),
            pltpu.VMEM((NZ, PROPS, 2 * WIDE), bf16),
            pltpu.VMEM((NZ, PROPS, 2 * WIDE), bf16),
            pltpu.VMEM((NKV, 1, WIDE), f32),
            pltpu.VMEM((SEQS, PROPS, WIDE), bf16),
            pltpu.VMEM((PROPS, 2 * WIDE), bf16),
            pltpu.VMEM((SEQS, PROPS, WIDE), bf16),
            pltpu.VMEM((SEQS, 1, WIDE), f32),
            pltpu.VMEM((NKV + 1, PROPS, WIDE), bf16),
            pltpu.VMEM((NKV + 1, 1, WIDE), f32),
            pltpu.VMEM((PROPS, WIDE), bf16),
            pltpu.VMEM((tp_count, SEQS // tp_count, PROPS, WIDE), bf16),
            pltpu.VMEM((WIDE, WIDE), f32),
            dma((14,)),
            dma((11,)),
            dma((9,)),
            dma((NZ,)),
            dma((tp_count,)),
            pltpu.SemaphoreType.REGULAR,
        ],
        compiler_params=pltpu.CompilerParams(
            collective_id=0, has_side_effects=True, vmem_limit_bytes=24 << 20
        ),
        name="tree_step",
    )(
        *(
            pltpu.with_memory_space_constraint(x, pltpu.HBM)
            for x in (
                tokens.T, norm_gain.reshape(1, width), w_query, w_key, w_value, w_gate.T, w_out.T,
                keys_cache, values_cache, cum_gates, gate_bias, prior_len, accepted, parents.T,
            )
        )
    )

    def held(x):
        return pltpu.with_memory_space_constraint(x, pltpu.VMEM)

    return pl.pallas_call(
        write_kernel,
        out_shape=(
            jax.ShapeDtypeStruct((out_rows, columns), bf16),
            jax.ShapeDtypeStruct(keys_cache.shape, bf16),
            jax.ShapeDtypeStruct(values_cache.shape, bf16),
        ),
        in_specs=[vmem, vmem, smem, vmem, vmem],
        out_specs=(any_, any_, any_),
        scratch_shapes=[dma((2,)), dma],
        compiler_params=pltpu.CompilerParams(vmem_limit_bytes=8 << 20),
        name="cache_write",
    )(
        held(mixed),
        held(new),
        pltpu.with_memory_space_constraint(filled, pltpu.SMEM),
        held(keys_held),
        held(values_held),
    )


def solution(mesh):
    in_specs = (
        P(None, "kv"),
        P("kv"),
        P("kv", "tp"),
        P("kv", "tp"),
        P("kv", "tp"),
        P(),
        P(),
        P("tp", "kv"),
        P(None, "kv", "tp"),
        P(None, "kv", "tp"),
        P(None, "tp", "kv"),
        P(),
        P(),
        P(),
    )
    out_specs = (P("tp", "kv"), P(None, "kv", "tp"), P(None, "kv", "tp"))
    return jax.shard_map(
        shards, mesh=mesh, in_specs=in_specs, out_specs=out_specs, check_vma=False
    )
```

```python
import functools

import jax
import jax.numpy as jnp
from jax import lax
from jax.experimental import pallas as pl
from jax.experimental.pallas import tpu as pltpu
from jax.sharding import PartitionSpec as P

D = 2048
HEAD = 64
PROPS = 16
SEQS = 24
NZ, NX = 8, 4
NKV = NZ * NX
WIDE = 128
MASKED = 1e30
NORM_EPS = 1e-06
FIRST_WRITER = 4

f32, bf16 = jnp.float32, jnp.bfloat16


def iota(shape, dim):
    return lax.broadcasted_iota(jnp.int32, shape, dim)


def dot_nt(a, b):
    return lax.dot_general(a, b, (((1,), (1,)), ((), ())), preferred_element_type=f32)


def dot_nn(a, b):
    return lax.dot_general(a, b, (((1,), (0,)), ((), ())), preferred_element_type=f32)


def far_first(i):
    return 4 + (1 - 2 * lax.rem(i, 2)) * lax.div(i + 1, 2)


def sequence_at(z, x):
    return lax.rem(z, 4) + 4 * x + 16 * lax.div(z, 4)


def split_heads(rows):
    lane = iota((2 * PROPS, WIDE), 1)
    sub = iota((2 * PROPS, WIDE), 0)
    both = jnp.concatenate([rows, rows], axis=0)
    return jnp.where((lane < HEAD) == (sub < PROPS), both, 0.0).astype(bf16)


def join_heads(rows):
    lane = iota((PROPS, WIDE), 1)
    return jnp.where(lane < HEAD, rows[:PROPS], rows[PROPS:])


def as_row(tops, sums):
    lane = iota((2 * PROPS, WIDE), 1)
    sub = iota((2 * PROPS, WIDE), 0)
    spread = jnp.where(lane == sub, tops, jnp.where(lane == sub + 2 * PROPS, sums, 0.0))
    return jnp.sum(spread, axis=0, keepdims=True)


def as_column(row, start):
    lane = iota((PROPS, WIDE), 1)
    sub = iota((PROPS, WIDE), 0)
    return jnp.sum(jnp.where(lane == sub + start, row, 0.0), axis=1, keepdims=True)


def step_kernel(
    tp_count,
    tok_hbm,
    gain_hbm,
    wq_hbm,
    wk_hbm,
    wv_hbm,
    wg_hbm,
    wo_hbm,
    keys_hbm,
    values_hbm,
    cum_hbm,
    bias_hbm,
    prior_hbm,
    accepted_hbm,
    parents_hbm,
    mixed_ref,
    new_ref,
    keys,
    values,
    filled_ref,
    bias_ref,
    prior_ref,
    accepted_ref,
    parents_ref,
    tok,
    gain,
    wq,
    wk,
    wv,
    wg,
    wo,
    keys_t,
    cum,
    part_q,
    part_n,
    part_s,
    got_q,
    got_x,
    sum_x,
    got_n,
    got_s,
    queries,
    own_new,
    out_v,
    out_s,
    got_v,
    got_m,
    own_rows,
    got_rows,
    reach,
    local_sems,
    send_sems,
    recv_sems,
    query_sems,
    row_sems,
    planes_in,
):
    me = lax.axis_index("kv")
    tp = lax.axis_index("tp")
    my_z, my_x = lax.div(me, NX), lax.rem(me, NX)
    owner = sequence_at(my_z, my_x) < SEQS
    own_b = lax.min(sequence_at(my_z, my_x), SEQS - 1)
    broad = my_x < 2
    per = SEQS // tp_count
    own_to = lax.div(own_b, per)
    half = max(1, tp_count // 2)
    length = keys.shape[1]
    offset = me * length
    heads = 2

    barrier = pltpu.get_barrier_semaphore()

    @pl.when(owner)
    def _():
        @pl.loop(0, NZ)
        def _(i):
            z = lax.rem(my_z + far_first(i), NZ)
            for k in range(NX):
                peer = z * NX + lax.rem(my_x + (2, 1, 3, 0)[k], NX)

                @pl.when(peer != me)
                def _():
                    pl.semaphore_signal(barrier, inc=1, device_id={"kv": peer})

    @pl.when(jnp.logical_not(owner))
    def _():
        for k in range(1, NX):
            peer = my_z * NX + lax.rem(my_x + k, NX)
            pl.semaphore_signal(barrier, inc=1, device_id={"kv": peer})

    @pl.loop(0, tp_count - 1)
    def _(i):
        pl.semaphore_signal(barrier, inc=1, device_id={"tp": lax.rem(tp + i + 1, tp_count)})

    gate_block = pl.multiple_of(lax.div(me, 2) * WIDE, WIDE)
    pairs = (
        (parents_hbm, parents_ref),
        (bias_hbm, bias_ref),
        (prior_hbm, prior_ref),
        (accepted_hbm, accepted_ref),
        (tok_hbm, tok),
        (gain_hbm, gain),
        (wg_hbm.at[:, pl.ds(gate_block, WIDE)], wg),
        (wq_hbm, wq),
        (wk_hbm, wk),
        (wv_hbm, wv),
        (cum_hbm, cum),
        (keys_hbm, keys),
        (values_hbm, values),
        (wo_hbm, wo.at[tp]),
    )
    loads = [pltpu.make_async_copy(a, b, local_sems.at[i]) for i, (a, b) in enumerate(pairs)]
    for load in loads:
        load.start()

    loads[0].wait()

    @pl.when(owner)
    def _():
        lane = iota((PROPS, WIDE), 1)
        sub = iota((PROPS, WIDE), 0)
        parent = jnp.full((PROPS, WIDE), -1, jnp.int32)
        for j in range(PROPS):
            parent = jnp.where(sub == j, parents_ref[j, own_b], parent)
        seen = jnp.where((lane == sub) | (lane == parent), 1.0, 0.0)
        rest = jnp.zeros((WIDE - PROPS, WIDE), f32)
        for _ in range(4):
            square = jnp.concatenate([seen, rest], axis=0).astype(bf16)
            seen = jnp.minimum(dot_nn(seen.astype(bf16), square), 1.0)
        reach[...] = jnp.concatenate([seen, rest], axis=0)

    with jax.named_scope("wait_inputs"):
        for load in loads[4:10]:
            load.wait()
    x = tok[...].astype(f32)
    width = x.shape[0]
    eye = iota((width, width), 0) == iota((width, width), 1)
    gain_col = jnp.sum(jnp.where(eye, gain[...], 0.0), axis=1, keepdims=True)
    square_row = jnp.sum(x * x, axis=0, keepdims=True)
    scaled_t = x * gain_col
    scaled = jnp.transpose(scaled_t).astype(bf16)
    gate_w = wg[...].astype(f32)
    gate_w = jnp.where(lax.rem(me, 2) == 0, gate_w[:, :width], gate_w[:, width:]).astype(bf16)
    gates = dot_nn(gate_w, scaled_t.astype(bf16))
    gate_row = iota(gates.shape, 0)
    rows = [square_row] + [
        jnp.sum(jnp.where(gate_row == heads * tp + h, gates, 0.0), axis=0, keepdims=True)
        for h in range(heads)
    ]
    sub, lane = iota((8, WIDE), 0), iota((8, WIDE), 1)
    for j in range(3):
        tile = jnp.zeros((8, WIDE), f32)
        for k, row in enumerate(rows):
            part = row[:, j * WIDE : (j + 1) * WIDE]
            part = pltpu.roll(jnp.broadcast_to(part, (8, WIDE)), k * PROPS, 1)
            tile = jnp.where(sub == k, part, tile)
        for c in range(8):
            moved = pltpu.roll(tile, (WIDE - c * PROPS) % WIDE, 1)
            moved = jnp.where(lax.shift_right_logical(lane, 4) == sub, moved, 0.0)
            part_s[8 * j + c] = jnp.sum(moved, axis=0, keepdims=True)
    part_q[...] = dot_nn(scaled, wq[...]).astype(bf16).reshape(SEQS, PROPS, WIDE)
    part_n[:, :, :WIDE] = dot_nn(scaled, wk[...]).astype(bf16).reshape(SEQS, PROPS, WIDE)
    part_n[:, :, WIDE:] = dot_nn(scaled, wv[...]).astype(bf16).reshape(SEQS, PROPS, WIDE)

    with jax.named_scope("barrier"):
        beside = jnp.where(my_z >= 4, 2, 0)
        pl.semaphore_wait(barrier, SEQS - 1 + beside + tp_count - 1)

    def remote(src, dst, send, recv, where):
        return pltpu.make_async_remote_copy(
            src_ref=src, dst_ref=dst, send_sem=send, recv_sem=recv, device_id=where
        )

    def to_owners(body):
        @pl.loop(0, NZ)
        def _(i):
            z = lax.rem(my_z + far_first(i), NZ)
            for x_at in range(NX):
                peer = z * NX + x_at
                b = sequence_at(z, x_at)

                @pl.when(jnp.logical_and(b < SEQS, peer != me))
                def _():
                    body(lax.min(b, SEQS - 1), peer)

    def to_everyone(body):
        @pl.loop(0, NZ)
        def _(i):
            z = lax.rem(my_z + far_first(i), NZ)
            for k in range(NX):
                body(z * NX + lax.rem(my_x + (2, 1, 3, 0)[k], NX), i)

    def to_all(body):
        def other(peer, i):
            @pl.when(peer != me)
            def _():
                body(peer, i)

        to_everyone(other)

    def send_queries(b, peer):
        remote(part_q.at[b], got_q.at[me], send_sems.at[0], recv_sems.at[0], {"kv": peer}).start()
        remote(part_s.at[b], got_s.at[me], send_sems.at[1], recv_sems.at[1], {"kv": peer}).start()

    def along_x(body):
        @pl.loop(0, NZ)
        def _(z):
            for x_at in range(NX):
                b = sequence_at(z, x_at)

                @pl.when(b < SEQS)
                def _():
                    body(lax.min(b, SEQS - 1), z, x_at)

    def in_column(body):
        @pl.loop(0, NZ)
        def _(i):
            z = lax.rem(my_z + far_first(i), NZ)
            b = sequence_at(z, my_x)

            @pl.when(b < SEQS)
            def _():
                body(lax.min(b, SEQS - 1), z)

    def send_new(b, z, x_at):
        slot = NX * z + my_x

        @pl.when(x_at != my_x)
        def _():
            there = {"kv": my_z * NX + x_at}
            remote(
                part_n.at[b], got_x.at[slot], send_sems.at[2], recv_sems.at[2], there
            ).start()

        @pl.when(x_at == my_x)
        def _():
            got_x[slot] = part_n[b]

    def pass_new(b, z):
        total = jnp.sum(got_x[pl.ds(NX * z, NX)].astype(f32), axis=0)
        sum_x[z] = total.astype(bf16)

    def send_sums(b, z):
        @pl.when(z != my_z)
        def _():
            there = {"kv": z * NX + my_x}
            remote(
                sum_x.at[z], got_n.at[my_z], send_sems.at[9], recv_sems.at[3], there
            ).start()

        @pl.when(z == my_z)
        def _():
            got_n[my_z] = sum_x[z]

    with jax.named_scope("send_parts"):
        to_owners(send_queries)

    loads[13].wait()

    @pl.loop(0, tp_count - 1)
    def _(i):
        there = {"tp": lax.rem(tp + i + 1, tp_count)}
        remote(wo.at[tp], wo.at[tp], send_sems.at[8], recv_sems.at[5], there).start()

    along_x(send_new)

    with jax.named_scope("wait_cache"):
        for load in (loads[1], loads[2], loads[3], loads[10], loads[11]):
            load.wait()
    positions = offset + iota((1, length), 1)

    for b in range(SEQS):
        filled_ref[b] = prior_ref[b] + accepted_ref[b]

    with jax.named_scope("prepare"):

        @pl.loop(0, SEQS)
        def _(b):
            filled = prior_ref[b] + accepted_ref[b]
            gates_b = cum[b]
            last = jnp.sum(
                jnp.where(positions == filled - 1, gates_b, 0.0), axis=1, keepdims=True
            )
            cum[b] = jnp.where(positions < filled, gates_b, MASKED)
            lane = iota((1, WIDE), 1)
            row = jnp.where(lane == 64, last[0:1], 0.0) + jnp.where(lane == 65, last[1:2], 0.0)
            out_s[b] = row
            keys_t[b] = jnp.transpose(keys[b])

    def arrived(ref, count, sem):
        some = ref.at[pl.ds(0, count)]
        pltpu.make_async_copy(some, some, sem).wait()

    sent = arrived

    def of_column(ref, count, other, sem):
        @pl.when(broad)
        def _():
            arrived(ref, count, sem)

        @pl.when(jnp.logical_not(broad))
        def _():
            arrived(ref, other, sem)

    def all_arrived(ref, sem):
        arrived(ref, NKV - 1, sem)

    def own_inverse(sums):
        return lax.rsqrt(as_column(sums, 0) / D + NORM_EPS)

    @pl.when(owner)
    def _():
        got_q[me] = part_q[own_b]
        got_s[me] = part_s[own_b]
        with jax.named_scope("wait_parts"):
            all_arrived(got_s, recv_sems.at[1])
            all_arrived(got_q, recv_sems.at[0])
        sums = jnp.sum(got_s[...], axis=0)
        inverse = own_inverse(sums)
        total = jnp.sum(got_q[...].astype(f32), axis=0)
        rounded = (inverse * total).astype(bf16).astype(f32)
        queries[own_b] = (rounded * HEAD**-0.5).astype(bf16)

        def send(peer, i):
            step = lax.rem(far_first(i), 4)
            part = jnp.where(step == 0, 0, jnp.where(step == 2, 2, 1))
            remote(
                queries.at[own_b],
                queries.at[own_b],
                send_sems.at[3],
                query_sems.at[part],
                {"kv": peer},
            ).start()

        with jax.named_scope("send_queries"):
            to_all(send)

        @pl.loop(0, tp_count - 1)
        def _(i):
            there = {"tp": lax.rem(tp + i + 1, tp_count)}
            pl.semaphore_signal(planes_in, inc=1, device_id=there)

    with jax.named_scope("pass_new"):
        of_column(got_x, 24, 12, recv_sems.at[2])
        in_column(pass_new)
        in_column(send_sums)

    with jax.named_scope("wait_cache"):
        loads[12].wait()

    def attend(steps):
        group = []
        for step in steps:
            z = lax.rem(my_z + step, 4)
            group += [(z + 4 * x_at, z * NX + x_at) for x_at in range(4)]
            group += [(z + 4 * x_at + 16, (z + 4) * NX + x_at) for x_at in range(2)]
        scores = []
        for b, _ in group:
            bias = cum[b]
            bias = jnp.concatenate(
                [jnp.broadcast_to(bias[h : h + 1], (PROPS, length)) for h in range(heads)], axis=0
            )
            query = split_heads(queries[b].astype(f32))
            scores.append(dot_nn(query, keys_t[b]) - bias)
        tops = [jnp.max(x, axis=1, keepdims=True) for x in scores]
        weights = [jnp.exp(x - top) for x, top in zip(scores, tops)]
        totals = [jnp.sum(x, axis=1, keepdims=True) for x in weights]
        blocks = [dot_nn(x.astype(bf16), values[b]) for x, (b, _) in zip(weights, group)]
        for k, (b, _) in enumerate(group):
            out_s[b] = out_s[b] + as_row(tops[k], totals[k])
            out_v[b] = join_heads(blocks[k]).astype(bf16)

        for b, peer in group:

            @pl.when(peer != me)
            def _():
                there = {"kv": peer}
                remote(
                    out_s.at[b], got_m.at[me], send_sems.at[4], recv_sems.at[7], there
                ).start()
                remote(
                    out_v.at[b], got_v.at[me], send_sems.at[5], recv_sems.at[4], there
                ).start()

    with jax.named_scope("wait_query"):

        @pl.when(owner)
        def _():
            arrived(queries, 5, query_sems.at[0])

        @pl.when(jnp.logical_not(owner))
        def _():
            arrived(queries, 6, query_sems.at[0])

    attend((0,))
    with jax.named_scope("wait_query"):
        arrived(queries, 12, query_sems.at[1])
    attend((1, 3))
    with jax.named_scope("wait_query"):
        arrived(queries, 6, query_sems.at[2])
    attend((2,))

    @pl.when(owner)
    def _():
        got_v[me] = out_v[own_b]
        got_m[me] = out_s[own_b]

        with jax.named_scope("wait_new"):
            arrived(got_n, NZ - 1, recv_sems.at[3])
        sums = jnp.sum(got_s[...], axis=0)
        inverse = own_inverse(sums)
        new = (inverse * jnp.sum(got_n[...].astype(f32), axis=0)).astype(bf16)
        own_new[...] = new

        for k in range(FIRST_WRITER, NZ):

            @pl.when(my_z != k)
            def _():
                there = {"kv": k * NX + my_x}
                remote(
                    own_new, new_ref.at[own_b], send_sems.at[6], recv_sems.at[6], there
                ).start()

        @pl.when(my_z >= FIRST_WRITER)
        def _():
            new_ref[own_b] = new

        seen = reach[...]
        seen_t = jnp.transpose(seen)[:PROPS]
        bias_rows = []
        for h in range(heads):
            logit = inverse * as_column(sums, PROPS * (h + 1)) + bias_ref[heads * tp + h]
            log_gate = jnp.minimum(logit, 0.0) - jnp.log1p(jnp.exp(-jnp.abs(logit)))
            tree_gate = jnp.sum(seen_t * log_gate, axis=0, keepdims=True)
            bias_rows.append(jnp.broadcast_to(tree_gate, (PROPS, WIDE)))
        rest = jnp.zeros((WIDE - PROPS, WIDE), bf16)
        new_keys = jnp.concatenate([new[:, :WIDE], rest], axis=0)
        new_values = jnp.concatenate([new[:, WIDE:], rest], axis=0)
        live = jnp.concatenate([seen[:PROPS], seen[:PROPS]], axis=0) > 0.5
        scores = dot_nt(split_heads(queries[own_b].astype(f32)), new_keys)
        scores = jnp.where(live, scores - jnp.concatenate(bias_rows, axis=0), -MASKED)
        top = jnp.max(scores, axis=1, keepdims=True)
        weights = jnp.where(live, jnp.exp(scores - top), 0.0)
        total = jnp.sum(weights, axis=1, keepdims=True)
        got_v[NKV] = join_heads(dot_nn(weights.astype(bf16), new_values)).astype(bf16)
        tree_row = as_row(top, total)

        with jax.named_scope("wait_stats"):
            all_arrived(got_m, recv_sems.at[7])
        lane = iota((1, WIDE), 1)
        stats = got_m[pl.ds(0, NKV)]
        ends = jnp.sum(stats, axis=0)
        last_0 = jnp.sum(jnp.where(lane == 64, ends, 0.0), axis=1, keepdims=True)
        last_1 = jnp.sum(jnp.where(lane == 65, ends, 0.0), axis=1, keepdims=True)
        shift = jnp.where(lane < PROPS, last_0, jnp.where(lane < 2 * PROPS, last_1, 0.0))
        got_m[NKV] = tree_row - shift
        stats = got_m[...]
        top = jnp.max(stats, axis=0, keepdims=True)
        held = lane.reshape(1, 1, WIDE) < 2 * PROPS
        factors = jnp.exp(jnp.where(held, stats - top, 0.0))
        sums_in = jnp.concatenate([stats[:, :, 32:], stats[:, :, :32]], axis=2)
        grand = jnp.sum(factors * sums_in, axis=0, keepdims=True)
        inverse_grand = 1.0 / jnp.where(held, grand, 1.0)[0]
        with jax.named_scope("wait_blocks"):
            all_arrived(got_v, recv_sems.at[4])
        first = iota((PROPS, WIDE), 1) < HEAD
        result = jnp.zeros((PROPS, WIDE), f32)
        for s in range(NKV + 1):
            share = factors[s]
            pair = jnp.where(first, as_column(share, 0), as_column(share, PROPS))
            result = result + pair * got_v[s].astype(f32)
        whole = jnp.where(first, as_column(inverse_grand, 0), as_column(inverse_grand, PROPS))
        own_rows[...] = (result * whole).astype(bf16)
        slot = lax.rem(own_b, per)

        if tp_count > 1:
            pl.semaphore_wait(planes_in, tp_count - 1)

        def send_rows(peer, step):
            @pl.when(jnp.logical_or(peer != me, own_to != tp))
            def _():
                remote(
                    own_rows,
                    got_rows.at[tp, slot],
                    send_sems.at[7],
                    row_sems.at[lax.div(lax.rem(tp - own_to + tp_count, tp_count), half)],
                    {"kv": peer, "tp": own_to},
                ).start()

        with jax.named_scope("send_rows"):
            to_everyone(send_rows)

        @pl.when(own_to == tp)
        def _():
            got_rows[tp, slot] = own_rows[...]

    @pl.when(my_z >= FIRST_WRITER)
    def _():
        with jax.named_scope("wait_column"):

            of_column(new_ref, 7, 4, recv_sems.at[6])

        def pass_on(b, z):
            for k in range(1, NX):
                there = {"kv": my_z * NX + lax.rem(my_x + k, NX)}
                remote(
                    new_ref.at[b], new_ref.at[b], send_sems.at[10], recv_sems.at[8], there
                ).start()

        in_column(pass_on)

    def sent_to_owners(count):
        sent(part_q, count, send_sems.at[0])
        sent(part_s, count, send_sems.at[1])
        sent(out_s, count, send_sems.at[4])
        sent(out_v, count, send_sems.at[5])
        of_column(got_x, 8 - SEQS + count, 4 - SEQS + count, send_sems.at[9])

    of_column(got_x, 16, 20, send_sems.at[2])

    @pl.when(owner)
    def _():
        sent_to_owners(SEQS - 1)
        sent(got_v, NKV - 1, send_sems.at[3])

        @pl.when(own_to == tp)
        def _():
            sent(got_v, NKV - 1, send_sems.at[7])

        @pl.when(own_to != tp)
        def _():
            sent(got_v, NKV, send_sems.at[7])

        @pl.when(my_z >= FIRST_WRITER)
        def _():
            sent(got_x, NZ - FIRST_WRITER - 1, send_sems.at[6])

        @pl.when(my_z < FIRST_WRITER)
        def _():
            sent(got_x, NZ - FIRST_WRITER, send_sems.at[6])

    @pl.when(jnp.logical_not(owner))
    def _():
        sent_to_owners(SEQS)

    if tp_count > 1:
        sent(wo, tp_count - 1, send_sems.at[8])

    @pl.when(my_z >= FIRST_WRITER)
    def _():
        of_column(got_x, 24, 12, send_sems.at[10])

        with jax.named_scope("wait_fresh"):
            of_column(new_ref, 16, 20, recv_sems.at[8])

    if tp_count > 1:
        arrived(wo, tp_count - 1, recv_sems.at[5])

    total = jnp.zeros((per * PROPS, wo.shape[1]), f32)
    mine_too = jnp.logical_and(owner, own_to == tp)
    for k in range(tp_count):
        plane = lax.rem(tp + k, tp_count)
        if k == 0:
            with jax.named_scope("wait_rows"):

                @pl.when(mine_too)
                def _():
                    arrived(got_v, half * per - 1, row_sems.at[0])

                @pl.when(jnp.logical_not(mine_too))
                def _():
                    arrived(got_v, half * per, row_sems.at[0])

        elif k == half:
            with jax.named_scope("wait_rows"):
                arrived(got_v, (tp_count - half) * per, row_sems.at[1])
        with jax.named_scope("project"):
            rows_in = got_rows[plane].reshape(per * PROPS, WIDE)
            total = total + dot_nt(rows_in, wo[plane])
    mixed_ref[...] = total.astype(bf16)


def write_kernel(
    mixed_in, new_ref, filled_ref, keys, values,
    mixed_out, keys_out, values_out, sems_out, sem_mixed,
):
    me = lax.axis_index("kv")
    length = keys.shape[1]
    both = ((keys, keys_out), (values, values_out))

    def copy_out(k, b):
        return pltpu.make_async_copy(both[k][0].at[b], both[k][1].at[b], sems_out.at[k])

    mixed = pltpu.make_async_copy(mixed_in, mixed_out, sem_mixed)
    mixed.start()

    @pl.loop(0, SEQS)
    def _(b):
        start = filled_ref[b] - me * length

        @pl.when((start > -PROPS) & (start < length))
        def _():
            base = jnp.clip(lax.shift_right_arithmetic(start, 4), 0, length // PROPS - 2) * PROPS
            rows = pl.ds(pl.multiple_of(base, PROPS), 2 * PROPS)
            slot = iota((2 * PROPS, PROPS), 0) + (base - start)
            pick = jnp.where(slot == iota((2 * PROPS, PROPS), 1), 1.0, 0.0).astype(bf16)
            placed = dot_nn(pick, new_ref[b])
            at = iota((2 * PROPS, WIDE), 0) + (base - start)
            inside = (at >= 0) & (at < PROPS)
            for k in range(2):
                held = both[k][0]
                old = held[b, rows, :].astype(f32)
                fresh = placed[:, k * WIDE : (k + 1) * WIDE]
                held[b, rows, :] = jnp.where(inside, fresh, old).astype(bf16)

        for k in range(2):
            copy_out(k, b).start()

    with jax.named_scope("write_wait"):

        for k in range(2):
            pltpu.make_async_copy(both[k][0], both[k][1], sems_out.at[k]).wait()

    mixed.wait()


def on_chip(shape, dtype):
    return pltpu.VMEM(shape, dtype)


def scalars(shape, dtype):
    return pltpu.SMEM(shape, dtype)


def shards(
    tokens, norm_gain, w_query, w_key, w_value, w_gate, gate_bias, w_out,
    keys_cache, values_cache, cum_gates, prior_len, accepted, parents,
):
    tp_count = lax.axis_size("tp")
    rows, width = tokens.shape
    columns = w_out.shape[1]
    length = keys_cache.shape[1]
    any_ = pl.BlockSpec(memory_space=pl.ANY)
    smem = pl.BlockSpec(memory_space=pltpu.SMEM)
    vmem = pl.BlockSpec(memory_space=pltpu.VMEM)
    out_rows = rows // tp_count
    dma = pltpu.SemaphoreType.DMA
    mixed, new, keys_held, values_held, filled = pl.pallas_call(
        functools.partial(step_kernel, tp_count),
        out_shape=(
            on_chip((out_rows, columns), bf16),
            on_chip((SEQS, PROPS, 2 * WIDE), bf16),
            on_chip(keys_cache.shape, bf16),
            on_chip(values_cache.shape, bf16),
            scalars(prior_len.shape, jnp.int32),
        ),
        in_specs=[pl.BlockSpec(memory_space=pltpu.HBM)] * 14,
        out_specs=(vmem, vmem, vmem, vmem, smem),
        scratch_shapes=[
            pltpu.SMEM(gate_bias.shape, f32),
            pltpu.SMEM(prior_len.shape, jnp.int32),
            pltpu.SMEM(accepted.shape, jnp.int32),
            pltpu.SMEM(parents.shape[::-1], jnp.int32),
            pltpu.VMEM((width, rows), bf16),
            pltpu.VMEM((1, width), f32),
            pltpu.VMEM((width, WIDE), bf16),
            pltpu.VMEM((width, WIDE), bf16),
            pltpu.VMEM((width, WIDE), bf16),
            pltpu.VMEM((w_gate.shape[1], WIDE), bf16),
            pltpu.VMEM((tp_count, columns, WIDE), bf16),
            pltpu.VMEM((SEQS, WIDE, length), bf16),
            pltpu.VMEM(cum_gates.shape, f32),
            pltpu.VMEM((SEQS, PROPS, WIDE), bf16),
            pltpu.VMEM((SEQS, PROPS, 2 * WIDE), bf16),
            pltpu.VMEM((SEQS, 1, WIDE), f32),
            pltpu.VMEM((NKV, PROPS, WIDE), bf16),
            pltpu.VMEM((NZ * NX, PROPS, 2 * WIDE), bf16),
            pltpu.VMEM((NZ, PROPS, 2 * WIDE), bf16),
            pltpu.VMEM((NZ, PROPS, 2 * WIDE), bf16),
            pltpu.VMEM((NKV, 1, WIDE), f32),
            pltpu.VMEM((SEQS, PROPS, WIDE), bf16),
            pltpu.VMEM((PROPS, 2 * WIDE), bf16),
            pltpu.VMEM((SEQS, PROPS, WIDE), bf16),
            pltpu.VMEM((SEQS, 1, WIDE), f32),
            pltpu.VMEM((NKV + 1, PROPS, WIDE), bf16),
            pltpu.VMEM((NKV + 1, 1, WIDE), f32),
            pltpu.VMEM((PROPS, WIDE), bf16),
            pltpu.VMEM((tp_count, SEQS // tp_count, PROPS, WIDE), bf16),
            pltpu.VMEM((WIDE, WIDE), f32),
            dma((14,)),
            dma((11,)),
            dma((9,)),
            dma((3,)),
            dma((2,)),
            pltpu.SemaphoreType.REGULAR,
        ],
        compiler_params=pltpu.CompilerParams(
            collective_id=0, has_side_effects=True, vmem_limit_bytes=24 << 20
        ),
        name="tree_step",
    )(
        *(
            pltpu.with_memory_space_constraint(x, pltpu.HBM)
            for x in (
                tokens.T, norm_gain.reshape(1, width), w_query, w_key, w_value, w_gate.T, w_out.T,
                keys_cache, values_cache, cum_gates, gate_bias, prior_len, accepted, parents.T,
            )
        )
    )

    def held(x):
        return pltpu.with_memory_space_constraint(x, pltpu.VMEM)

    return pl.pallas_call(
        write_kernel,
        out_shape=(
            jax.ShapeDtypeStruct((out_rows, columns), bf16),
            jax.ShapeDtypeStruct(keys_cache.shape, bf16),
            jax.ShapeDtypeStruct(values_cache.shape, bf16),
        ),
        in_specs=[vmem, vmem, smem, vmem, vmem],
        out_specs=(any_, any_, any_),
        scratch_shapes=[dma((2,)), dma],
        compiler_params=pltpu.CompilerParams(vmem_limit_bytes=8 << 20),
        name="cache_write",
    )(
        held(mixed),
        held(new),
        pltpu.with_memory_space_constraint(filled, pltpu.SMEM),
        held(keys_held),
        held(values_held),
    )


def solution(mesh):
    in_specs = (
        P(None, "kv"),
        P("kv"),
        P("kv", "tp"),
        P("kv", "tp"),
        P("kv", "tp"),
        P(),
        P(),
        P("tp", "kv"),
        P(None, "kv", "tp"),
        P(None, "kv", "tp"),
        P(None, "tp", "kv"),
        P(),
        P(),
        P(),
    )
    out_specs = (P("tp", "kv"), P(None, "kv", "tp"), P(None, "kv", "tp"))
    return jax.shard_map(
        shards, mesh=mesh, in_specs=in_specs, out_specs=out_specs, check_vma=False
    )
```

```python
import functools

import jax
import jax.numpy as jnp
from jax import lax
from jax.experimental import pallas as pl
from jax.experimental.pallas import tpu as pltpu
from jax.sharding import PartitionSpec as P

D = 2048
HEAD = 64
PROPS = 16
SEQS = 24
NZ, NX = 8, 4
NKV = NZ * NX
WIDE = 128
MASKED = 1e30
NORM_EPS = 1e-06
FIRST_WRITER = 4

f32, bf16 = jnp.float32, jnp.bfloat16


def iota(shape, dim):
    return lax.broadcasted_iota(jnp.int32, shape, dim)


def dot_nt(a, b):
    return lax.dot_general(a, b, (((1,), (1,)), ((), ())), preferred_element_type=f32)


def dot_nn(a, b):
    return lax.dot_general(a, b, (((1,), (0,)), ((), ())), preferred_element_type=f32)


def far_first(i):
    return 4 + (1 - 2 * lax.rem(i, 2)) * lax.div(i + 1, 2)


def sequence_at(z, x):
    return lax.rem(z, 4) + 4 * x + 16 * lax.div(z, 4)


def split_heads(rows):
    lane = iota((2 * PROPS, WIDE), 1)
    sub = iota((2 * PROPS, WIDE), 0)
    both = jnp.concatenate([rows, rows], axis=0)
    return jnp.where((lane < HEAD) == (sub < PROPS), both, 0.0).astype(bf16)


def join_heads(rows):
    lane = iota((PROPS, WIDE), 1)
    return jnp.where(lane < HEAD, rows[:PROPS], rows[PROPS:])


def as_row(tops, sums):
    lane = iota((2 * PROPS, WIDE), 1)
    sub = iota((2 * PROPS, WIDE), 0)
    spread = jnp.where(lane == sub, tops, jnp.where(lane == sub + 2 * PROPS, sums, 0.0))
    return jnp.sum(spread, axis=0, keepdims=True)


def as_column(row, start):
    lane = iota((PROPS, WIDE), 1)
    sub = iota((PROPS, WIDE), 0)
    return jnp.sum(jnp.where(lane == sub + start, row, 0.0), axis=1, keepdims=True)


def step_kernel(
    tp_count,
    tok_hbm,
    gain_hbm,
    wq_hbm,
    wk_hbm,
    wv_hbm,
    wg_hbm,
    wo_hbm,
    keys_hbm,
    values_hbm,
    cum_hbm,
    bias_hbm,
    prior_hbm,
    accepted_hbm,
    parents_hbm,
    mixed_ref,
    new_ref,
    keys,
    values,
    filled_ref,
    bias_ref,
    prior_ref,
    accepted_ref,
    parents_ref,
    tok,
    gain,
    wq,
    wk,
    wv,
    wg,
    wo,
    keys_t,
    cum,
    part_q,
    part_n,
    part_s,
    got_q,
    got_x,
    sum_x,
    got_n,
    got_s,
    queries,
    own_new,
    out_v,
    out_s,
    got_v,
    got_m,
    own_rows,
    got_rows,
    reach,
    local_sems,
    send_sems,
    recv_sems,
    query_sems,
    row_sems,
    planes_in,
):
    me = lax.axis_index("kv")
    tp = lax.axis_index("tp")
    my_z, my_x = lax.div(me, NX), lax.rem(me, NX)
    owner = sequence_at(my_z, my_x) < SEQS
    own_b = lax.min(sequence_at(my_z, my_x), SEQS - 1)
    broad = my_x < 2
    per = SEQS // tp_count
    own_to = lax.div(own_b, per)
    half = max(1, tp_count // 2)
    length = keys.shape[1]
    offset = me * length
    heads = 2

    barrier = pltpu.get_barrier_semaphore()

    @pl.when(owner)
    def _():
        @pl.loop(0, NZ)
        def _(i):
            z = lax.rem(my_z + far_first(i), NZ)
            for k in range(NX):
                peer = z * NX + lax.rem(my_x + (2, 1, 3, 0)[k], NX)

                @pl.when(peer != me)
                def _():
                    pl.semaphore_signal(barrier, inc=1, device_id={"kv": peer})

    @pl.when(jnp.logical_not(owner))
    def _():
        for k in range(1, NX):
            peer = my_z * NX + lax.rem(my_x + k, NX)
            pl.semaphore_signal(barrier, inc=1, device_id={"kv": peer})

    @pl.loop(0, tp_count - 1)
    def _(i):
        pl.semaphore_signal(barrier, inc=1, device_id={"tp": lax.rem(tp + i + 1, tp_count)})

    gate_block = pl.multiple_of(lax.div(me, 2) * WIDE, WIDE)
    pairs = (
        (parents_hbm, parents_ref),
        (bias_hbm, bias_ref),
        (prior_hbm, prior_ref),
        (accepted_hbm, accepted_ref),
        (tok_hbm, tok),
        (gain_hbm, gain),
        (wg_hbm.at[:, pl.ds(gate_block, WIDE)], wg),
        (wq_hbm, wq),
        (wk_hbm, wk),
        (wv_hbm, wv),
        (cum_hbm, cum),
        (keys_hbm, keys),
        (values_hbm, values),
        (wo_hbm, wo.at[tp]),
    )
    loads = [pltpu.make_async_copy(a, b, local_sems.at[i]) for i, (a, b) in enumerate(pairs)]
    for load in loads:
        load.start()

    loads[0].wait()

    @pl.when(owner)
    def _():
        lane = iota((PROPS, WIDE), 1)
        sub = iota((PROPS, WIDE), 0)
        parent = jnp.full((PROPS, WIDE), -1, jnp.int32)
        for j in range(PROPS):
            parent = jnp.where(sub == j, parents_ref[j, own_b], parent)
        seen = jnp.where((lane == sub) | (lane == parent), 1.0, 0.0)
        rest = jnp.zeros((WIDE - PROPS, WIDE), f32)
        for _ in range(4):
            square = jnp.concatenate([seen, rest], axis=0).astype(bf16)
            seen = jnp.minimum(dot_nn(seen.astype(bf16), square), 1.0)
        reach[...] = jnp.concatenate([seen, rest], axis=0)

    with jax.named_scope("wait_inputs"):
        for load in loads[4:10]:
            load.wait()
    x = tok[...].astype(f32)
    width = x.shape[0]
    eye = iota((width, width), 0) == iota((width, width), 1)
    gain_col = jnp.sum(jnp.where(eye, gain[...], 0.0), axis=1, keepdims=True)
    square_row = jnp.sum(x * x, axis=0, keepdims=True)
    scaled_t = x * gain_col
    scaled = jnp.transpose(scaled_t).astype(bf16)
    gate_w = wg[...].astype(f32)
    gate_w = jnp.where(lax.rem(me, 2) == 0, gate_w[:, :width], gate_w[:, width:]).astype(bf16)
    gates = dot_nn(gate_w, scaled_t.astype(bf16))
    gate_row = iota(gates.shape, 0)
    rows = [square_row] + [
        jnp.sum(jnp.where(gate_row == heads * tp + h, gates, 0.0), axis=0, keepdims=True)
        for h in range(heads)
    ]
    sub, lane = iota((8, WIDE), 0), iota((8, WIDE), 1)
    for j in range(3):
        tile = jnp.zeros((8, WIDE), f32)
        for k, row in enumerate(rows):
            part = row[:, j * WIDE : (j + 1) * WIDE]
            part = pltpu.roll(jnp.broadcast_to(part, (8, WIDE)), k * PROPS, 1)
            tile = jnp.where(sub == k, part, tile)
        for c in range(8):
            moved = pltpu.roll(tile, (WIDE - c * PROPS) % WIDE, 1)
            moved = jnp.where(lax.shift_right_logical(lane, 4) == sub, moved, 0.0)
            part_s[8 * j + c] = jnp.sum(moved, axis=0, keepdims=True)
    part_q[...] = dot_nn(scaled, wq[...]).astype(bf16).reshape(SEQS, PROPS, WIDE)
    part_n[:, :, :WIDE] = dot_nn(scaled, wk[...]).astype(bf16).reshape(SEQS, PROPS, WIDE)
    part_n[:, :, WIDE:] = dot_nn(scaled, wv[...]).astype(bf16).reshape(SEQS, PROPS, WIDE)

    with jax.named_scope("barrier"):
        beside = jnp.where(my_z >= 4, 2, 0)
        pl.semaphore_wait(barrier, SEQS - 1 + beside + tp_count - 1)

    def remote(src, dst, send, recv, where):
        return pltpu.make_async_remote_copy(
            src_ref=src, dst_ref=dst, send_sem=send, recv_sem=recv, device_id=where
        )

    def to_owners(body):
        @pl.loop(0, NZ)
        def _(i):
            z = lax.rem(my_z + far_first(i), NZ)
            for x_at in range(NX):
                peer = z * NX + x_at
                b = sequence_at(z, x_at)

                @pl.when(jnp.logical_and(b < SEQS, peer != me))
                def _():
                    body(lax.min(b, SEQS - 1), peer)

    def to_everyone(body):
        @pl.loop(0, NZ)
        def _(i):
            z = lax.rem(my_z + far_first(i), NZ)
            for k in range(NX):
                body(z * NX + lax.rem(my_x + (2, 1, 3, 0)[k], NX), i)

    def to_all(body):
        def other(peer, i):
            @pl.when(peer != me)
            def _():
                body(peer, i)

        to_everyone(other)

    def send_queries(b, peer):
        remote(part_q.at[b], got_q.at[me], send_sems.at[0], recv_sems.at[0], {"kv": peer}).start()
        remote(part_s.at[b], got_s.at[me], send_sems.at[1], recv_sems.at[1], {"kv": peer}).start()

    def along_x(body):
        @pl.loop(0, NZ)
        def _(z):
            for x_at in range(NX):
                b = sequence_at(z, x_at)

                @pl.when(b < SEQS)
                def _():
                    body(lax.min(b, SEQS - 1), z, x_at)

    def in_column(body):
        @pl.loop(0, NZ)
        def _(i):
            z = lax.rem(my_z + far_first(i), NZ)
            b = sequence_at(z, my_x)

            @pl.when(b < SEQS)
            def _():
                body(lax.min(b, SEQS - 1), z)

    def send_new(b, z, x_at):
        slot = NX * z + my_x

        @pl.when(x_at != my_x)
        def _():
            there = {"kv": my_z * NX + x_at}
            remote(
                part_n.at[b], got_x.at[slot], send_sems.at[2], recv_sems.at[2], there
            ).start()

        @pl.when(x_at == my_x)
        def _():
            got_x[slot] = part_n[b]

    def pass_new(b, z):
        total = jnp.sum(got_x[pl.ds(NX * z, NX)].astype(f32), axis=0)
        sum_x[z] = total.astype(bf16)

    def send_sums(b, z):
        @pl.when(z != my_z)
        def _():
            there = {"kv": z * NX + my_x}
            remote(
                sum_x.at[z], got_n.at[my_z], send_sems.at[9], recv_sems.at[3], there
            ).start()

        @pl.when(z == my_z)
        def _():
            got_n[my_z] = sum_x[z]

    with jax.named_scope("send_parts"):
        to_owners(send_queries)

    loads[13].wait()

    @pl.loop(0, tp_count - 1)
    def _(i):
        there = {"tp": lax.rem(tp + i + 1, tp_count)}
        remote(wo.at[tp], wo.at[tp], send_sems.at[8], recv_sems.at[5], there).start()

    along_x(send_new)

    with jax.named_scope("wait_cache"):
        for load in (loads[1], loads[2], loads[3], loads[10], loads[11]):
            load.wait()
    positions = offset + iota((1, length), 1)

    for b in range(SEQS):
        filled_ref[b] = prior_ref[b] + accepted_ref[b]

    with jax.named_scope("prepare"):

        @pl.loop(0, SEQS)
        def _(b):
            filled = prior_ref[b] + accepted_ref[b]
            gates_b = cum[b]
            last = jnp.sum(
                jnp.where(positions == filled - 1, gates_b, 0.0), axis=1, keepdims=True
            )
            cum[b] = jnp.where(positions < filled, gates_b, MASKED)
            lane = iota((1, WIDE), 1)
            row = jnp.where(lane == 64, last[0:1], 0.0) + jnp.where(lane == 65, last[1:2], 0.0)
            out_s[b] = row
            keys_t[b] = jnp.transpose(keys[b])

    def arrived(ref, count, sem):
        some = ref.at[pl.ds(0, count)]
        pltpu.make_async_copy(some, some, sem).wait()

    sent = arrived

    def of_column(ref, count, other, sem):
        @pl.when(broad)
        def _():
            arrived(ref, count, sem)

        @pl.when(jnp.logical_not(broad))
        def _():
            arrived(ref, other, sem)

    def all_arrived(ref, sem):
        arrived(ref, NKV - 1, sem)

    def own_inverse(sums):
        return lax.rsqrt(as_column(sums, 0) / D + NORM_EPS)

    @pl.when(owner)
    def _():
        got_q[me] = part_q[own_b]
        got_s[me] = part_s[own_b]
        with jax.named_scope("wait_parts"):
            all_arrived(got_s, recv_sems.at[1])
            all_arrived(got_q, recv_sems.at[0])
        sums = jnp.sum(got_s[...], axis=0)
        inverse = own_inverse(sums)
        total = jnp.sum(got_q[...].astype(f32), axis=0)
        rounded = (inverse * total).astype(bf16).astype(f32)
        queries[own_b] = (rounded * HEAD**-0.5).astype(bf16)

        def send(peer, i):
            step = lax.rem(far_first(i), 4)
            part = jnp.where(step == 0, 0, 1)
            remote(
                queries.at[own_b],
                queries.at[own_b],
                send_sems.at[3],
                query_sems.at[part],
                {"kv": peer},
            ).start()

        with jax.named_scope("send_queries"):
            to_all(send)

        @pl.loop(0, tp_count - 1)
        def _(i):
            there = {"tp": lax.rem(tp + i + 1, tp_count)}
            pl.semaphore_signal(planes_in, inc=1, device_id=there)

    with jax.named_scope("pass_new"):
        of_column(got_x, 24, 12, recv_sems.at[2])
        in_column(pass_new)
        in_column(send_sums)

    with jax.named_scope("wait_cache"):
        loads[12].wait()

    def attend(steps):
        group = []
        for step in steps:
            z = lax.rem(my_z + step, 4)
            group += [(z + 4 * x_at, z * NX + x_at) for x_at in range(4)]
            group += [(z + 4 * x_at + 16, (z + 4) * NX + x_at) for x_at in range(2)]
        scores = []
        for b, _ in group:
            bias = cum[b]
            bias = jnp.concatenate(
                [jnp.broadcast_to(bias[h : h + 1], (PROPS, length)) for h in range(heads)], axis=0
            )
            query = split_heads(queries[b].astype(f32))
            scores.append(dot_nn(query, keys_t[b]) - bias)
        tops = [jnp.max(x, axis=1, keepdims=True) for x in scores]
        weights = [jnp.exp(x - top) for x, top in zip(scores, tops)]
        totals = [jnp.sum(x, axis=1, keepdims=True) for x in weights]
        blocks = [dot_nn(x.astype(bf16), values[b]) for x, (b, _) in zip(weights, group)]
        for k, (b, _) in enumerate(group):
            out_s[b] = out_s[b] + as_row(tops[k], totals[k])
            out_v[b] = join_heads(blocks[k]).astype(bf16)

        for b, peer in group:

            @pl.when(peer != me)
            def _():
                there = {"kv": peer}
                remote(
                    out_s.at[b], got_m.at[me], send_sems.at[4], recv_sems.at[7], there
                ).start()
                remote(
                    out_v.at[b], got_v.at[me], send_sems.at[5], recv_sems.at[4], there
                ).start()

    with jax.named_scope("wait_query"):

        @pl.when(owner)
        def _():
            arrived(queries, 5, query_sems.at[0])

        @pl.when(jnp.logical_not(owner))
        def _():
            arrived(queries, 6, query_sems.at[0])

    attend((0,))
    with jax.named_scope("wait_query"):
        arrived(queries, 18, query_sems.at[1])
    attend((1, 3, 2))

    @pl.when(owner)
    def _():
        got_v[me] = out_v[own_b]
        got_m[me] = out_s[own_b]

        with jax.named_scope("wait_new"):
            arrived(got_n, NZ - 1, recv_sems.at[3])
        sums = jnp.sum(got_s[...], axis=0)
        inverse = own_inverse(sums)
        new = (inverse * jnp.sum(got_n[...].astype(f32), axis=0)).astype(bf16)
        own_new[...] = new

        for k in range(FIRST_WRITER, NZ):

            @pl.when(my_z != k)
            def _():
                there = {"kv": k * NX + my_x}
                remote(
                    own_new, new_ref.at[own_b], send_sems.at[6], recv_sems.at[6], there
                ).start()

        @pl.when(my_z >= FIRST_WRITER)
        def _():
            new_ref[own_b] = new

        seen = reach[...]
        seen_t = jnp.transpose(seen)[:PROPS]
        bias_rows = []
        for h in range(heads):
            logit = inverse * as_column(sums, PROPS * (h + 1)) + bias_ref[heads * tp + h]
            log_gate = jnp.minimum(logit, 0.0) - jnp.log1p(jnp.exp(-jnp.abs(logit)))
            tree_gate = jnp.sum(seen_t * log_gate, axis=0, keepdims=True)
            bias_rows.append(jnp.broadcast_to(tree_gate, (PROPS, WIDE)))
        rest = jnp.zeros((WIDE - PROPS, WIDE), bf16)
        new_keys = jnp.concatenate([new[:, :WIDE], rest], axis=0)
        new_values = jnp.concatenate([new[:, WIDE:], rest], axis=0)
        live = jnp.concatenate([seen[:PROPS], seen[:PROPS]], axis=0) > 0.5
        scores = dot_nt(split_heads(queries[own_b].astype(f32)), new_keys)
        scores = jnp.where(live, scores - jnp.concatenate(bias_rows, axis=0), -MASKED)
        top = jnp.max(scores, axis=1, keepdims=True)
        weights = jnp.where(live, jnp.exp(scores - top), 0.0)
        total = jnp.sum(weights, axis=1, keepdims=True)
        got_v[NKV] = join_heads(dot_nn(weights.astype(bf16), new_values)).astype(bf16)
        tree_row = as_row(top, total)

        with jax.named_scope("wait_stats"):
            all_arrived(got_m, recv_sems.at[7])
        lane = iota((1, WIDE), 1)
        stats = got_m[pl.ds(0, NKV)]
        ends = jnp.sum(stats, axis=0)
        last_0 = jnp.sum(jnp.where(lane == 64, ends, 0.0), axis=1, keepdims=True)
        last_1 = jnp.sum(jnp.where(lane == 65, ends, 0.0), axis=1, keepdims=True)
        shift = jnp.where(lane < PROPS, last_0, jnp.where(lane < 2 * PROPS, last_1, 0.0))
        got_m[NKV] = tree_row - shift
        stats = got_m[...]
        top = jnp.max(stats, axis=0, keepdims=True)
        held = lane.reshape(1, 1, WIDE) < 2 * PROPS
        factors = jnp.exp(jnp.where(held, stats - top, 0.0))
        sums_in = jnp.concatenate([stats[:, :, 32:], stats[:, :, :32]], axis=2)
        grand = jnp.sum(factors * sums_in, axis=0, keepdims=True)
        inverse_grand = 1.0 / jnp.where(held, grand, 1.0)[0]
        with jax.named_scope("wait_blocks"):
            all_arrived(got_v, recv_sems.at[4])
        first = iota((PROPS, WIDE), 1) < HEAD
        result = jnp.zeros((PROPS, WIDE), f32)
        for s in range(NKV + 1):
            share = factors[s]
            pair = jnp.where(first, as_column(share, 0), as_column(share, PROPS))
            result = result + pair * got_v[s].astype(f32)
        whole = jnp.where(first, as_column(inverse_grand, 0), as_column(inverse_grand, PROPS))
        own_rows[...] = (result * whole).astype(bf16)
        slot = lax.rem(own_b, per)

        if tp_count > 1:
            pl.semaphore_wait(planes_in, tp_count - 1)

        def send_rows(peer, step):
            @pl.when(jnp.logical_or(peer != me, own_to != tp))
            def _():
                remote(
                    own_rows,
                    got_rows.at[tp, slot],
                    send_sems.at[7],
                    row_sems.at[lax.div(lax.rem(tp - own_to + tp_count, tp_count), half)],
                    {"kv": peer, "tp": own_to},
                ).start()

        with jax.named_scope("send_rows"):
            to_everyone(send_rows)

        @pl.when(own_to == tp)
        def _():
            got_rows[tp, slot] = own_rows[...]

    @pl.when(my_z >= FIRST_WRITER)
    def _():
        with jax.named_scope("wait_column"):

            of_column(new_ref, 7, 4, recv_sems.at[6])

        def pass_on(b, z):
            for k in range(1, NX):
                there = {"kv": my_z * NX + lax.rem(my_x + k, NX)}
                remote(
                    new_ref.at[b], new_ref.at[b], send_sems.at[10], recv_sems.at[8], there
                ).start()

        in_column(pass_on)

    def sent_to_owners(count):
        sent(part_q, count, send_sems.at[0])
        sent(part_s, count, send_sems.at[1])
        sent(out_s, count, send_sems.at[4])
        sent(out_v, count, send_sems.at[5])
        of_column(got_x, 8 - SEQS + count, 4 - SEQS + count, send_sems.at[9])

    of_column(got_x, 16, 20, send_sems.at[2])

    @pl.when(owner)
    def _():
        sent_to_owners(SEQS - 1)
        sent(got_v, NKV - 1, send_sems.at[3])

        @pl.when(own_to == tp)
        def _():
            sent(got_v, NKV - 1, send_sems.at[7])

        @pl.when(own_to != tp)
        def _():
            sent(got_v, NKV, send_sems.at[7])

        @pl.when(my_z >= FIRST_WRITER)
        def _():
            sent(got_x, NZ - FIRST_WRITER - 1, send_sems.at[6])

        @pl.when(my_z < FIRST_WRITER)
        def _():
            sent(got_x, NZ - FIRST_WRITER, send_sems.at[6])

    @pl.when(jnp.logical_not(owner))
    def _():
        sent_to_owners(SEQS)

    if tp_count > 1:
        sent(wo, tp_count - 1, send_sems.at[8])

    @pl.when(my_z >= FIRST_WRITER)
    def _():
        of_column(got_x, 24, 12, send_sems.at[10])

        with jax.named_scope("wait_fresh"):
            of_column(new_ref, 16, 20, recv_sems.at[8])

    if tp_count > 1:
        arrived(wo, tp_count - 1, recv_sems.at[5])

    total = jnp.zeros((per * PROPS, wo.shape[1]), f32)
    mine_too = jnp.logical_and(owner, own_to == tp)
    for k in range(tp_count):
        plane = lax.rem(tp + k, tp_count)
        if k == 0:
            with jax.named_scope("wait_rows"):

                @pl.when(mine_too)
                def _():
                    arrived(got_v, half * per - 1, row_sems.at[0])

                @pl.when(jnp.logical_not(mine_too))
                def _():
                    arrived(got_v, half * per, row_sems.at[0])

        elif k == half:
            with jax.named_scope("wait_rows"):
                arrived(got_v, (tp_count - half) * per, row_sems.at[1])
        with jax.named_scope("project"):
            rows_in = got_rows[plane].reshape(per * PROPS, WIDE)
            total = total + dot_nt(rows_in, wo[plane])
    mixed_ref[...] = total.astype(bf16)


def write_kernel(
    mixed_in, new_ref, filled_ref, keys, values,
    mixed_out, keys_out, values_out, sems_out, sem_mixed,
):
    me = lax.axis_index("kv")
    length = keys.shape[1]
    both = ((keys, keys_out), (values, values_out))

    def copy_out(k, b):
        return pltpu.make_async_copy(both[k][0].at[b], both[k][1].at[b], sems_out.at[k])

    mixed = pltpu.make_async_copy(mixed_in, mixed_out, sem_mixed)
    mixed.start()

    @pl.loop(0, SEQS)
    def _(b):
        start = filled_ref[b] - me * length

        @pl.when((start > -PROPS) & (start < length))
        def _():
            base = jnp.clip(lax.shift_right_arithmetic(start, 4), 0, length // PROPS - 2) * PROPS
            rows = pl.ds(pl.multiple_of(base, PROPS), 2 * PROPS)
            slot = iota((2 * PROPS, PROPS), 0) + (base - start)
            pick = jnp.where(slot == iota((2 * PROPS, PROPS), 1), 1.0, 0.0).astype(bf16)
            placed = dot_nn(pick, new_ref[b])
            at = iota((2 * PROPS, WIDE), 0) + (base - start)
            inside = (at >= 0) & (at < PROPS)
            for k in range(2):
                held = both[k][0]
                old = held[b, rows, :].astype(f32)
                fresh = placed[:, k * WIDE : (k + 1) * WIDE]
                held[b, rows, :] = jnp.where(inside, fresh, old).astype(bf16)

        for k in range(2):
            copy_out(k, b).start()

    with jax.named_scope("write_wait"):

        for k in range(2):
            pltpu.make_async_copy(both[k][0], both[k][1], sems_out.at[k]).wait()

    mixed.wait()


def on_chip(shape, dtype):
    return pltpu.VMEM(shape, dtype)


def scalars(shape, dtype):
    return pltpu.SMEM(shape, dtype)


def shards(
    tokens, norm_gain, w_query, w_key, w_value, w_gate, gate_bias, w_out,
    keys_cache, values_cache, cum_gates, prior_len, accepted, parents,
):
    tp_count = lax.axis_size("tp")
    rows, width = tokens.shape
    columns = w_out.shape[1]
    length = keys_cache.shape[1]
    any_ = pl.BlockSpec(memory_space=pl.ANY)
    smem = pl.BlockSpec(memory_space=pltpu.SMEM)
    vmem = pl.BlockSpec(memory_space=pltpu.VMEM)
    out_rows = rows // tp_count
    dma = pltpu.SemaphoreType.DMA
    mixed, new, keys_held, values_held, filled = pl.pallas_call(
        functools.partial(step_kernel, tp_count),
        out_shape=(
            on_chip((out_rows, columns), bf16),
            on_chip((SEQS, PROPS, 2 * WIDE), bf16),
            on_chip(keys_cache.shape, bf16),
            on_chip(values_cache.shape, bf16),
            scalars(prior_len.shape, jnp.int32),
        ),
        in_specs=[pl.BlockSpec(memory_space=pltpu.HBM)] * 14,
        out_specs=(vmem, vmem, vmem, vmem, smem),
        scratch_shapes=[
            pltpu.SMEM(gate_bias.shape, f32),
            pltpu.SMEM(prior_len.shape, jnp.int32),
            pltpu.SMEM(accepted.shape, jnp.int32),
            pltpu.SMEM(parents.shape[::-1], jnp.int32),
            pltpu.VMEM((width, rows), bf16),
            pltpu.VMEM((1, width), f32),
            pltpu.VMEM((width, WIDE), bf16),
            pltpu.VMEM((width, WIDE), bf16),
            pltpu.VMEM((width, WIDE), bf16),
            pltpu.VMEM((w_gate.shape[1], WIDE), bf16),
            pltpu.VMEM((tp_count, columns, WIDE), bf16),
            pltpu.VMEM((SEQS, WIDE, length), bf16),
            pltpu.VMEM(cum_gates.shape, f32),
            pltpu.VMEM((SEQS, PROPS, WIDE), bf16),
            pltpu.VMEM((SEQS, PROPS, 2 * WIDE), bf16),
            pltpu.VMEM((SEQS, 1, WIDE), f32),
            pltpu.VMEM((NKV, PROPS, WIDE), bf16),
            pltpu.VMEM((NZ * NX, PROPS, 2 * WIDE), bf16),
            pltpu.VMEM((NZ, PROPS, 2 * WIDE), bf16),
            pltpu.VMEM((NZ, PROPS, 2 * WIDE), bf16),
            pltpu.VMEM((NKV, 1, WIDE), f32),
            pltpu.VMEM((SEQS, PROPS, WIDE), bf16),
            pltpu.VMEM((PROPS, 2 * WIDE), bf16),
            pltpu.VMEM((SEQS, PROPS, WIDE), bf16),
            pltpu.VMEM((SEQS, 1, WIDE), f32),
            pltpu.VMEM((NKV + 1, PROPS, WIDE), bf16),
            pltpu.VMEM((NKV + 1, 1, WIDE), f32),
            pltpu.VMEM((PROPS, WIDE), bf16),
            pltpu.VMEM((tp_count, SEQS // tp_count, PROPS, WIDE), bf16),
            pltpu.VMEM((WIDE, WIDE), f32),
            dma((14,)),
            dma((11,)),
            dma((9,)),
            dma((2,)),
            dma((2,)),
            pltpu.SemaphoreType.REGULAR,
        ],
        compiler_params=pltpu.CompilerParams(
            collective_id=0, has_side_effects=True, vmem_limit_bytes=24 << 20
        ),
        name="tree_step",
    )(
        *(
            pltpu.with_memory_space_constraint(x, pltpu.HBM)
            for x in (
                tokens.T, norm_gain.reshape(1, width), w_query, w_key, w_value, w_gate.T, w_out.T,
                keys_cache, values_cache, cum_gates, gate_bias, prior_len, accepted, parents.T,
            )
        )
    )

    def held(x):
        return pltpu.with_memory_space_constraint(x, pltpu.VMEM)

    return pl.pallas_call(
        write_kernel,
        out_shape=(
            jax.ShapeDtypeStruct((out_rows, columns), bf16),
            jax.ShapeDtypeStruct(keys_cache.shape, bf16),
            jax.ShapeDtypeStruct(values_cache.shape, bf16),
        ),
        in_specs=[vmem, vmem, smem, vmem, vmem],
        out_specs=(any_, any_, any_),
        scratch_shapes=[dma((2,)), dma],
        compiler_params=pltpu.CompilerParams(vmem_limit_bytes=8 << 20),
        name="cache_write",
    )(
        held(mixed),
        held(new),
        pltpu.with_memory_space_constraint(filled, pltpu.SMEM),
        held(keys_held),
        held(values_held),
    )


def solution(mesh):
    in_specs = (
        P(None, "kv"),
        P("kv"),
        P("kv", "tp"),
        P("kv", "tp"),
        P("kv", "tp"),
        P(),
        P(),
        P("tp", "kv"),
        P(None, "kv", "tp"),
        P(None, "kv", "tp"),
        P(None, "tp", "kv"),
        P(),
        P(),
        P(),
    )
    out_specs = (P("tp", "kv"), P(None, "kv", "tp"), P(None, "kv", "tp"))
    return jax.shard_map(
        shards, mesh=mesh, in_specs=in_specs, out_specs=out_specs, check_vma=False
    )
```
